32 devices in a mesh: sp: 4 (over z), fs: 4 (over y, x), tp: 2 (over core).
Axes of the slice: x: 2, y: 2, z: 4, core: 2. Of those that a mesh axis runs over, the one named last changes fastest.
Arguments:
- tokens: bfloat16 [4, 1024, 2048], P('fs', 'sp', 'tp'), may hold values from -6 to 6
- norm_gain: float32 [2048], replicated, may hold values from 0.1 to 1.9
- lin_query: bfloat16 [2048, 1024], P(None, ('fs', 'tp')), may hold values from -0.125 to 0.125
- lin_key: bfloat16 [2048, 1024], P(None, ('fs', 'tp')), may hold values from -0.125 to 0.125
- lin_value: bfloat16 [2048, 2048], P(None, ('fs', 'tp')), may hold values from -0.125 to 0.125
- lin_decay: bfloat16 [2048, 1024], P(None, ('fs', 'tp')), may hold values from -0.125 to 0.125
- decay_bias: float32 [1024], replicated, may hold values from -0.5 to 8.5
- decay_shift: bfloat16 [2, 4, 1024], P(None, 'fs', 'sp'), may hold values from -1.4 to 1.5, as said below
- soft_query: bfloat16 [2048, 2048], P(None, ('fs', 'tp')), may hold values from -0.190034947 to 0.190034947
- soft_key: bfloat16 [2048, 2048], P(None, ('fs', 'tp')), may hold values from -1.9887378 to 1.9887378
- soft_value: bfloat16 [2048, 2048], P(None, ('fs', 'tp')), may hold values from -0.125 to 0.125
- soft_lambda: float32 [8], replicated, may hold values from 0.3 to 0.8
- lin_gain: float32 [256], replicated, may hold values from 0.1 to 1.9
- soft_gain: float32 [256], replicated, may hold values from 0.1 to 1.9
- lin_out: bfloat16 [2048, 2048], P(('fs', 'tp')), may hold values from -0.09375 to 0.09375
- soft_out: bfloat16 [2048, 2048], P(('fs', 'tp')), may hold values from -0.09375 to 0.09375
Outputs:
- mixed: bfloat16 [4, 1024, 2048], P('fs', 'sp', 'tp')
- log_mass: float32 [8, 2, 4, 1024], P(('fs', 'tp'), None, None, 'sp')
The draws below stay inside these ranges and needn't reach their ends.
Inputs may be any that keep to these rules, and one draw needn't show every extreme that they name: `decay_shift`: row 1 is never positive.
All inputs are finite; a program needn't handle non-finite values.
Results may differ from the reference program's by a relative error of at most 0.02.
Values may be sent and summed in bfloat16 or wider, within the bound.
A program may use at most 192 MiB of HBM per device.

```python
import jax
import jax.numpy as jnp
from jax import lax

D = 2048
GLA_HEADS = 8
GLA_KEY = 128
GLA_VALUE = 256
DIFF_HEADS = 8
DIFF_HEAD = 128
DIFF_VALUE = 256
BLOCK = 64
TOK_DEV = 256
SEQUENCE_LENGTH = 1024
BATCH_SEQUENCES = 4


def draw_decay_bias(key, part):
    slow_share = 0.5
    slow_heads = jax.random.bernoulli(jax.random.fold_in(key, 201), slow_share, (GLA_HEADS,)).astype(jnp.float32)
    jitter = jax.random.uniform(jax.random.fold_in(key, 202), (GLA_HEADS, GLA_KEY), jnp.float32, -0.5, 0.5)
    return (8.0 * slow_heads[:, None] + jitter).reshape(GLA_HEADS * GLA_KEY)


def draw_decay_shift(key, part):
    level_count = SEQUENCE_LENGTH // TOK_DEV
    levels = jax.random.uniform(jax.random.fold_in(key, 301), (BATCH_SEQUENCES, level_count), jnp.float32, -0.8, 0.8)
    jitter = jax.random.uniform(jax.random.fold_in(key, 302), (BATCH_SEQUENCES, SEQUENCE_LENGTH), jnp.float32, -0.3, 0.3)
    gate_vector_row = jnp.repeat(levels, TOK_DEV, axis=1) + jitter
    spurt_position = jax.random.randint(jax.random.fold_in(key, 303), (BATCH_SEQUENCES, 3), 0, SEQUENCE_LENGTH)
    spurt_depth = jnp.log(jax.random.uniform(jax.random.fold_in(key, 304), (BATCH_SEQUENCES, 3), jnp.float32, 0.5, 0.8))
    match_count = jnp.arange(SEQUENCE_LENGTH, dtype=jnp.int32)[None, None, :] == spurt_position[:, :, None]
    spurt_row = jnp.sum(jnp.where(match_count, spurt_depth[:, :, None], 0.0), axis=1)
    return jnp.stack([gate_vector_row, spurt_row]).astype(jnp.bfloat16)


def query_table(key):
    raw_draw = jnp.clip(jax.random.normal(jax.random.fold_in(key, 101), (D, DIFF_HEADS * 2 * DIFF_HEAD), jnp.float32), -6.0, 6.0)
    return raw_draw * (2.0 / D) ** 0.5


def draw_soft_query(key, part):
    return query_table(key).astype(jnp.bfloat16)


def draw_soft_key(key, part):
    own_draw = jnp.clip(jax.random.normal(jax.random.fold_in(key, 102), (D, DIFF_HEADS * 2 * DIFF_HEAD), jnp.float32), -6.0, 6.0)
    own_draw = own_draw * (2.0 / D) ** 0.5
    result = own_draw
    return result.astype(jnp.bfloat16)


def block_scale(rng, extent, pieces, smallest, top_value):
    factor_of = 1.0
    for position, shards_of in pieces:
        steps = jax.random.uniform(jax.random.fold_in(jax.random.fold_in(rng, 6), position), (shards_of,), jnp.float32, smallest / len(pieces), top_value / len(pieces))
        factor_of = factor_of * jnp.repeat(jnp.exp(steps), extent[position] // shards_of).reshape((-1,) + (1,) * (len(extent) - 1 - position))
    return factor_of


def gaussian(stream_key, dims, scale, most, pieces=(), kind=jnp.bfloat16):
    drawn = scale * jax.random.normal(stream_key, dims, jnp.float32)
    if pieces:
        drawn = drawn * block_scale(stream_key, dims, pieces, -0.22, 0.18)
    return jnp.clip(drawn, -most, most).astype(kind)


def setup_inputs(seed: int = 0) -> dict:
    keys = jax.random.split(jax.random.key(seed), 17)
    tokens = gaussian(keys[0], (BATCH_SEQUENCES, SEQUENCE_LENGTH, D), 1.0, 6.0, ((0, 4), (1, 4), (2, 2)))
    norm_gain = jnp.clip(1.0 + 0.18 * jax.random.normal(keys[1], (D,), jnp.float32), 0.1, 1.9)
    lin_query = gaussian(keys[2], (D, GLA_HEADS * GLA_KEY), D ** -0.5, 0.125, ((1, 8),))
    lin_key = gaussian(keys[3], (D, GLA_HEADS * GLA_KEY), D ** -0.5, 0.125, ((1, 8),))
    lin_value = gaussian(keys[4], (D, GLA_HEADS * GLA_VALUE), D ** -0.5, 0.125, ((1, 8),))
    lin_decay = gaussian(keys[5], (D, GLA_HEADS * GLA_KEY), D ** -0.5, 0.125, ((1, 8),))
    decay_bias = draw_decay_bias(jax.random.fold_in(keys[16], 71), 0)
    decay_shift = draw_decay_shift(jax.random.fold_in(keys[16], 71), 0)
    soft_query = draw_soft_query(jax.random.fold_in(keys[16], 71), 0)
    soft_key = draw_soft_key(jax.random.fold_in(keys[16], 71), 0)
    soft_value = gaussian(keys[10], (D, DIFF_HEADS * DIFF_VALUE), D ** -0.5, 0.125, ((1, 8),))
    soft_lambda = jnp.clip(jax.random.uniform(keys[11], (DIFF_HEADS,), jnp.float32, 0.3, 0.8), 0.3, 0.8)
    lin_gain = jnp.clip(1.0 + 0.18 * jax.random.normal(keys[12], (GLA_VALUE,), jnp.float32), 0.1, 1.9)
    soft_gain = jnp.clip(1.0 + 0.18 * jax.random.normal(keys[13], (DIFF_VALUE,), jnp.float32), 0.1, 1.9)
    lin_out = gaussian(keys[14], (GLA_HEADS * GLA_VALUE, D), (GLA_HEADS * GLA_VALUE + DIFF_HEADS * DIFF_VALUE) ** -0.5, 0.09375, ((0, 8),))
    soft_out = gaussian(keys[15], (DIFF_HEADS * DIFF_VALUE, D), (GLA_HEADS * GLA_VALUE + DIFF_HEADS * DIFF_VALUE) ** -0.5, 0.09375, ((0, 8),))
    return dict(tokens=tokens, norm_gain=norm_gain, lin_query=lin_query, lin_key=lin_key, lin_value=lin_value, lin_decay=lin_decay, decay_bias=decay_bias, decay_shift=decay_shift, soft_query=soft_query, soft_key=soft_key, soft_value=soft_value, soft_lambda=soft_lambda, lin_gain=lin_gain, soft_gain=soft_gain, lin_out=lin_out, soft_out=soft_out)


norm_eps = 1e-06
decay_tau = 16.0
rope_base = 500000.0
highest = lax.Precision.HIGHEST

def scaled_rms(values, norm_gain):
    return values * lax.rsqrt(lax.optimization_barrier(jnp.mean(values * values, axis=-1, keepdims=True)) + norm_eps) * norm_gain

def rotate(values, positions):
    half_dim = values.shape[-1] // 2
    inv_freq = jnp.power(jnp.float32(rope_base), -jnp.arange(half_dim, dtype=jnp.float32) * (2.0 / values.shape[-1]))
    angles = positions.astype(jnp.float32)[:, None] * inv_freq[None, :]
    cos_table = jnp.cos(angles)[:, None, None, :]
    sin_table = jnp.sin(angles)[:, None, None, :]
    widened = values.astype(jnp.float32)
    first_half = widened[..., :half_dim]
    second_half = widened[..., half_dim:]
    turned = jnp.concatenate([first_half * cos_table - second_half * sin_table, second_half * cos_table + first_half * sin_table], axis=-1)
    return turned.astype(jnp.bfloat16)

def block_pass(queries, key_rows, value_rows, log_decay, block_len):
    groups, length, heads, key_dim = queries.shape
    value_dim = value_rows.shape[-1]
    block_count = length // block_len

    def split(tensor):
        return tensor.reshape(groups, block_count, block_len, heads, tensor.shape[-1]).transpose(1, 0, 3, 2, 4)
    causal = jnp.tril(jnp.ones((block_len, block_len), dtype=bool))[:, :, None]

    def advance(carry, inputs):
        state_now, offset = carry
        query_blk, key_blk, value_blk, decay_blk = inputs
        cum_log = jnp.cumsum(decay_blk, axis=2)
        inner_part = jnp.einsum('bhcd,bhdv->bhcv', query_blk * jnp.exp(cum_log), state_now, precision=highest)
        decay_pair = jnp.exp(jnp.where(causal, cum_log[:, :, :, None, :] - cum_log[:, :, None, :, :], -jnp.inf))
        scores = lax.optimization_barrier(jnp.sum(query_blk[:, :, :, None, :] * key_blk[:, :, None, :, :] * decay_pair, axis=-1))
        local_part = jnp.einsum('bhij,bhjv->bhiv', scores, value_blk, precision=highest)
        last_log = cum_log[:, :, -1, :]
        state_now = jnp.exp(last_log)[..., None] * state_now + jnp.einsum('bhcd,bhcv->bhdv', key_blk * jnp.exp(last_log[:, :, None, :] - cum_log), value_blk, precision=highest)
        carried = query_blk * jnp.exp(offset[:, :, None, :] + cum_log)
        return ((state_now, offset + last_log), (inner_part + local_part, carried))
    start = (jnp.zeros((groups, heads, key_dim, value_dim), jnp.float32), jnp.zeros((groups, heads, key_dim), jnp.float32))
    (state_end, offset_end), (outs, carried) = lax.scan(advance, start, (split(queries), split(key_rows), split(value_rows), split(log_decay)))
    return (outs, carried, state_end, offset_end)

def reference(tokens, norm_gain, lin_query, lin_key, lin_value, lin_decay, decay_bias, decay_shift, soft_query, soft_key, soft_value, soft_lambda, lin_gain, soft_gain, lin_out, soft_out):
    seq_count, seq_len, model_width = tokens.shape
    widened = tokens.astype(jnp.float32)
    normed = scaled_rms(widened, norm_gain).astype(jnp.bfloat16)
    flat_rows = normed.reshape(seq_count * seq_len, model_width)

    def project(weight):
        return jnp.dot(flat_rows, weight, preferred_element_type=jnp.float32)
    shift_rows = decay_shift.astype(jnp.float32)
    lin_q = project(lin_query).astype(jnp.bfloat16).reshape(seq_count, seq_len, GLA_HEADS, GLA_KEY)
    lin_k = project(lin_key).astype(jnp.bfloat16).reshape(seq_count, seq_len, GLA_HEADS, GLA_KEY)
    lin_v = project(lin_value).astype(jnp.bfloat16).reshape(seq_count, seq_len, GLA_HEADS, GLA_VALUE)
    gate_input = project(lin_decay) + decay_bias[None, :] + shift_rows[0].reshape(seq_count * seq_len)[:, None]
    log_decay = jax.nn.log_sigmoid(gate_input) / decay_tau + shift_rows[1].reshape(seq_count * seq_len)[:, None]
    log_decay = log_decay.reshape(seq_count, seq_len, GLA_HEADS, GLA_KEY)
    outs, carried, state_end, offset_end = block_pass(lin_q.astype(jnp.float32), lin_k.astype(jnp.float32), lin_v.astype(jnp.float32), log_decay, BLOCK)
    lin_raw = outs.transpose(1, 0, 3, 2, 4).reshape(seq_count, seq_len, GLA_HEADS, GLA_VALUE)
    lin_mix = scaled_rms(lin_raw, lin_gain).astype(jnp.bfloat16).reshape(seq_count * seq_len, GLA_HEADS * GLA_VALUE)
    positions = jnp.arange(seq_len, dtype=jnp.int32)
    soft_q = rotate(project(soft_query).astype(jnp.bfloat16).reshape(seq_count, seq_len, DIFF_HEADS, 2, DIFF_HEAD), positions)
    soft_k = rotate(project(soft_key).astype(jnp.bfloat16).reshape(seq_count, seq_len, DIFF_HEADS, 2, DIFF_HEAD), positions)
    soft_v = project(soft_value).astype(jnp.bfloat16).reshape(seq_count, seq_len, DIFF_HEADS, DIFF_VALUE)
    block_count = seq_len // TOK_DEV
    scale = DIFF_HEAD ** (-0.5)
    key_pos = jnp.arange(seq_len, dtype=jnp.int32)

    def attend(flat_index):
        seq_id = flat_index // block_count
        blk_id = flat_index % block_count
        seq_queries = lax.dynamic_index_in_dim(soft_q, seq_id, 0, keepdims=False)
        query_blk = lax.dynamic_slice_in_dim(seq_queries, blk_id * TOK_DEV, TOK_DEV, 0)
        seq_keys = lax.dynamic_index_in_dim(soft_k, seq_id, 0, keepdims=False)
        seq_values = lax.dynamic_index_in_dim(soft_v, seq_id, 0, keepdims=False)
        scores = jnp.einsum('qhmd,khmd->hmqk', query_blk.astype(jnp.float32), seq_keys.astype(jnp.float32)) * scale
        query_pos = blk_id * TOK_DEV + jnp.arange(TOK_DEV, dtype=jnp.int32)
        scores = jnp.where(key_pos[None, :] <= query_pos[:, None], scores, -jnp.inf)
        top = lax.optimization_barrier(jnp.max(scores, axis=-1, keepdims=True))
        expo = jnp.exp(scores - top)
        total = lax.optimization_barrier(jnp.sum(expo, axis=-1, keepdims=True))
        probs = expo / total
        mass = top[..., 0] + jnp.log(total[..., 0])
        weights = (probs[:, 0] - soft_lambda[:, None, None] * probs[:, 1]).astype(jnp.bfloat16)
        mixed_blk = jnp.einsum('hqk,khv->hqv', weights.astype(jnp.float32), seq_values.astype(jnp.float32))
        return (mixed_blk, mass)
    soft_raw, mass = lax.map(attend, jnp.arange(seq_count * block_count, dtype=jnp.int32))
    soft_raw = soft_raw.reshape(seq_count, block_count, DIFF_HEADS, TOK_DEV, DIFF_VALUE).transpose(0, 1, 3, 2, 4)
    soft_raw = soft_raw.reshape(seq_count, seq_len, DIFF_HEADS, DIFF_VALUE)
    soft_mix = scaled_rms(soft_raw, soft_gain).astype(jnp.bfloat16).reshape(seq_count * seq_len, DIFF_HEADS * DIFF_VALUE)
    log_mass = mass.reshape(seq_count, block_count, DIFF_HEADS, 2, TOK_DEV).transpose(2, 3, 0, 1, 4)
    log_mass = log_mass.reshape(DIFF_HEADS, 2, seq_count, seq_len)
    summed = jnp.dot(lin_mix, lin_out, preferred_element_type=jnp.float32) + jnp.dot(soft_mix, soft_out, preferred_element_type=jnp.float32)
    mixed = summed.astype(jnp.bfloat16).reshape(seq_count, seq_len, model_width)
    return (mixed, log_mass)
```

```python
import functools

import jax
import jax.numpy as jnp
import numpy as np
from jax import lax
from jax.experimental import pallas as pl
from jax.experimental.pallas import tpu as pltpu
from jax.sharding import PartitionSpec as P

GLA_KEY = 128
GLA_VALUE = 256
DIFF_HEAD = 128
DIFF_VALUE = 256
BLOCK = 64


norm_eps = 1e-06
decay_tau = 16.0
rope_base = 500000.0
highest = lax.Precision.HIGHEST


def prefix(array, axis, join, neutral):
    place = lax.axis_index(axis)
    gathered = jax.tree.map(
        lambda a, kind: lax.all_gather(a.astype(kind), axis), array, (jnp.bfloat16, jnp.bfloat16)
    )
    state = jax.tree.map(lambda a, e: jnp.zeros_like(a) + jnp.asarray(e, a.dtype), array, neutral)

    def one(turn, state):
        return join(
            state,
            jax.tree.map(
                lambda a, own: lax.dynamic_index_in_dim(a, turn, 0, False).astype(own.dtype),
                gathered,
                array,
            ),
        )

    return lax.fori_loop(0, place, one, state)


def scaled_rms(values, norm_gain):
    return (
        values * lax.rsqrt(jnp.mean(values * values, axis=-1, keepdims=True) + norm_eps) * norm_gain
    )


def rotate(values, positions):
    half_dim = values.shape[-1] // 2
    inv_freq = jnp.power(
        jnp.float32(rope_base), -jnp.arange(half_dim, dtype=jnp.float32) * (2.0 / values.shape[-1])
    )
    angles = positions.astype(jnp.float32)[:, None] * inv_freq[None, :]
    cos_table = jnp.cos(angles)[:, None, None, :]
    sin_table = jnp.sin(angles)[:, None, None, :]
    widened = values.astype(jnp.float32)
    first_half = widened[..., :half_dim]
    second_half = widened[..., half_dim:]
    turned = jnp.concatenate(
        [
            first_half * cos_table - second_half * sin_table,
            second_half * cos_table + first_half * sin_table,
        ],
        axis=-1,
    )
    return turned.astype(jnp.bfloat16)


def block_pass(queries, key_rows, value_rows, log_decay, block_len):
    groups, length, heads, key_dim = queries.shape
    value_dim = value_rows.shape[-1]
    block_count = length // block_len

    def split(tensor):
        return tensor.reshape(groups, block_count, block_len, heads, tensor.shape[-1]).transpose(
            1, 0, 3, 2, 4
        )

    causal = jnp.tril(jnp.ones((block_len, block_len), dtype=bool))[:, :, None]

    def advance(carry, inputs):
        state_now, offset = carry
        query_blk, key_blk, value_blk, decay_blk = inputs
        cum_log = jnp.cumsum(decay_blk, axis=2)
        inner_part = jnp.einsum(
            "bhcd,bhdv->bhcv", query_blk * jnp.exp(cum_log), state_now, precision=highest
        )
        decay_pair = jnp.exp(
            jnp.where(causal, cum_log[:, :, :, None, :] - cum_log[:, :, None, :, :], -jnp.inf)
        )
        scores = jnp.sum(
            query_blk[:, :, :, None, :] * key_blk[:, :, None, :, :] * decay_pair, axis=-1
        )
        local_part = jnp.einsum("bhij,bhjv->bhiv", scores, value_blk, precision=highest)
        last_log = cum_log[:, :, -1, :]
        state_now = jnp.exp(last_log)[..., None] * state_now + jnp.einsum(
            "bhcd,bhcv->bhdv",
            key_blk * jnp.exp(last_log[:, :, None, :] - cum_log),
            value_blk,
            precision=highest,
        )
        carried = query_blk * jnp.exp(offset[:, :, None, :] + cum_log)
        return ((state_now, offset + last_log), (inner_part + local_part, carried))

    start = (
        jnp.zeros((groups, heads, key_dim, value_dim), jnp.float32),
        jnp.zeros((groups, heads, key_dim), jnp.float32),
    )
    (state_end, offset_end), (outs, carried) = lax.scan(
        advance, start, (split(queries), split(key_rows), split(value_rows), split(log_decay))
    )
    return (outs, carried, state_end, offset_end)


def project(rows, weight):
    lead_shape = rows.shape[:-1]
    flat_rows = rows.reshape(-1, rows.shape[-1])
    product = jnp.dot(flat_rows, weight, preferred_element_type=jnp.float32)
    return product.reshape(lead_shape + (weight.shape[1],))


def chain_join(earlier, later):
    return (earlier[0] * later[0], later[0][..., None] * earlier[1] + later[1])


def attend(queries, query_pos, reach, all_keys, all_values, soft_lambda, soft_gain, rows_dev):
    groups, query_rows, soft_heads = queries.shape[:3]
    block_total = all_keys.shape[1] // rows_dev
    scale = DIFF_HEAD ** (-0.5)

    def first_pass(block_id, carry):
        top_now, total_now, score_store = carry
        key_blk = lax.dynamic_slice_in_dim(all_keys, block_id * rows_dev, rows_dev, 1)
        raw_scores = (
            jnp.einsum("bqhmd,bkhmd->bhmqk", queries, key_blk, preferred_element_type=jnp.float32)
            * scale
        )
        key_pos = block_id * rows_dev + jnp.arange(rows_dev, dtype=jnp.int32)
        scores = jnp.where(key_pos[None, :] <= query_pos[:, None], raw_scores, -jnp.inf)
        top_next = jnp.maximum(top_now, jnp.max(scores, axis=-1))
        total_next = total_now * jnp.exp(top_now - top_next) + jnp.sum(
            jnp.exp(scores - top_next[..., None]), axis=-1
        )
        score_store = lax.dynamic_update_index_in_dim(score_store, scores, block_id, 0)
        return (top_next, total_next, score_store)

    stat_shape = (groups, soft_heads, 2, query_rows)
    store_init = jnp.full((block_total,) + stat_shape + (rows_dev,), -jnp.inf, jnp.float32)
    top_all, total_all, score_store = lax.fori_loop(
        0,
        reach,
        first_pass,
        (
            jnp.full(stat_shape, -jnp.inf, jnp.float32),
            jnp.zeros(stat_shape, jnp.float32),
            store_init,
        ),
    )
    mass = top_all + jnp.log(total_all)

    def second_pass(block_id, accum):
        scores = lax.dynamic_index_in_dim(score_store, block_id, 0, keepdims=False)
        probs = jnp.exp(scores - top_all[..., None]) / total_all[..., None]
        weights = (probs[:, :, 0] - soft_lambda[None, :, None, None] * probs[:, :, 1]).astype(
            jnp.bfloat16
        )
        value_blk = lax.dynamic_slice_in_dim(all_values, block_id * rows_dev, rows_dev, 1)
        return accum + jnp.einsum(
            "bhqk,bkhv->bhqv", weights, value_blk, preferred_element_type=jnp.float32
        )

    accum = lax.fori_loop(
        0, reach, second_pass, jnp.zeros((groups, soft_heads, query_rows, DIFF_VALUE), jnp.float32)
    )
    soft_mix = scaled_rms(accum, soft_gain).astype(jnp.bfloat16).transpose(0, 2, 1, 3)
    soft_mix = soft_mix.reshape(groups, query_rows, soft_heads * DIFF_VALUE)
    return (soft_mix, mass)


def mixers(
    normed,
    shift_rows,
    lin_query,
    lin_key,
    lin_value,
    lin_decay,
    decay_bias,
    soft_query,
    soft_key,
    soft_value,
    soft_lambda,
    lin_gain,
    soft_gain,
):
    groups, rows_dev, model_width = normed.shape
    lin_heads = lin_query.shape[1] // GLA_KEY
    soft_heads = soft_value.shape[1] // DIFF_VALUE
    place = lax.axis_index("sp")
    shift_wide = shift_rows.astype(jnp.float32)
    lin_q = (
        project(normed, lin_query)
        .astype(jnp.bfloat16)
        .reshape(groups, rows_dev, lin_heads, GLA_KEY)
    )
    lin_k = (
        project(normed, lin_key).astype(jnp.bfloat16).reshape(groups, rows_dev, lin_heads, GLA_KEY)
    )
    lin_v = (
        project(normed, lin_value)
        .astype(jnp.bfloat16)
        .reshape(groups, rows_dev, lin_heads, GLA_VALUE)
    )
    gate_input = project(normed, lin_decay) + decay_bias + shift_wide[0][:, :, None]
    log_decay = jax.nn.log_sigmoid(gate_input) / decay_tau + shift_wide[1][:, :, None]
    log_decay = log_decay.reshape(groups, rows_dev, lin_heads, GLA_KEY)
    outs, carried, state_end, offset_end = block_pass(
        lin_q.astype(jnp.float32),
        lin_k.astype(jnp.float32),
        lin_v.astype(jnp.float32),
        log_decay,
        BLOCK,
    )
    keep_in, state_in = prefix(
        (jnp.exp(offset_end), state_end),
        "sp",
        chain_join,
        (jnp.ones_like(offset_end), jnp.zeros_like(state_end)),
    )
    outs = outs + jnp.einsum("nbhcd,bhdv->nbhcv", carried, state_in, precision=highest)
    lin_raw = outs.transpose(1, 0, 3, 2, 4).reshape(groups, rows_dev, lin_heads, GLA_VALUE)
    lin_mix = (
        scaled_rms(lin_raw, lin_gain)
        .astype(jnp.bfloat16)
        .reshape(groups, rows_dev, lin_heads * GLA_VALUE)
    )
    positions = place * rows_dev + jnp.arange(rows_dev, dtype=jnp.int32)
    soft_q = rotate(
        project(normed, soft_query)
        .astype(jnp.bfloat16)
        .reshape(groups, rows_dev, soft_heads, 2, DIFF_HEAD),
        positions,
    )
    soft_k = rotate(
        project(normed, soft_key)
        .astype(jnp.bfloat16)
        .reshape(groups, rows_dev, soft_heads, 2, DIFF_HEAD),
        positions,
    )
    soft_v = (
        project(normed, soft_value)
        .astype(jnp.bfloat16)
        .reshape(groups, rows_dev, soft_heads, DIFF_VALUE)
    )
    all_keys, all_values = (
        lax.all_gather(soft_k, "sp", axis=1, tiled=True),
        lax.all_gather(soft_v, "sp", axis=1, tiled=True),
    )
    soft_mix, mass = attend(
        soft_q, positions, place + 1, all_keys, all_values, soft_lambda, soft_gain, rows_dev
    )
    return (lin_mix, soft_mix, mass)


def output_term(lin_mix, soft_mix, lin_out, soft_out, rows_dev, parts):
    col_width = lin_out.shape[1] // parts

    def term(start, row_count):
        pieces = []
        for turn_index in range(row_count // rows_dev):
            piece_id = (start + turn_index * rows_dev) // rows_dev
            seq_id = piece_id // parts
            part_id = piece_id % parts
            lin_rows = lax.dynamic_index_in_dim(lin_mix, seq_id, 0, keepdims=False)
            soft_rows = lax.dynamic_index_in_dim(soft_mix, seq_id, 0, keepdims=False)
            lin_cols = lax.dynamic_slice_in_dim(lin_out, part_id * col_width, col_width, 1)
            soft_cols = lax.dynamic_slice_in_dim(soft_out, part_id * col_width, col_width, 1)
            pieces.append(
                jnp.dot(lin_rows, lin_cols, preferred_element_type=jnp.float32)
                + jnp.dot(soft_rows, soft_cols, preferred_element_type=jnp.float32)
            )
        return jnp.concatenate(pieces, axis=0)

    return term


def shards(
    tokens,
    norm_gain,
    lin_query,
    lin_key,
    lin_value,
    lin_decay,
    decay_bias,
    decay_shift,
    soft_query,
    soft_key,
    soft_value,
    soft_lambda,
    lin_gain,
    soft_gain,
    lin_out,
    soft_out,
):
    rows_dev = tokens.shape[1]
    parts = lax.axis_size("tp")
    fs_size = lax.axis_size("fs")
    fs_index = lax.axis_index("fs")
    tp_index = lax.axis_index("tp")
    whole = lax.all_gather(tokens, "tp", axis=2, tiled=True).astype(jnp.float32)
    normed = scaled_rms(whole, norm_gain).astype(jnp.bfloat16)
    lambda_grid = soft_lambda.reshape(fs_size, parts, -1)
    bias_grid = decay_bias.reshape(fs_size, parts, -1)
    all_rows, all_shift = (
        lax.all_gather(normed, "fs", axis=0, tiled=True),
        lax.all_gather(decay_shift, "fs", axis=1, tiled=True),
    )
    head_lambda = lax.dynamic_index_in_dim(
        lax.dynamic_index_in_dim(lambda_grid, fs_index, 0, keepdims=False),
        tp_index,
        0,
        keepdims=False,
    )
    head_bias = lax.dynamic_index_in_dim(
        lax.dynamic_index_in_dim(bias_grid, fs_index, 0, keepdims=False),
        tp_index,
        0,
        keepdims=False,
    )
    lin_mix, soft_mix, mass = mixers(
        all_rows,
        all_shift,
        lin_query,
        lin_key,
        lin_value,
        lin_decay,
        head_bias,
        soft_query,
        soft_key,
        soft_value,
        head_lambda,
        lin_gain,
        soft_gain,
    )
    term = output_term(lin_mix, soft_mix, lin_out, soft_out, rows_dev, parts)
    summed = lax.psum_scatter(
        term(jnp.int32(0), rows_dev * lax.axis_size(("fs", "tp"))).astype(jnp.bfloat16),
        ("fs", "tp"),
        scatter_dimension=0,
        tiled=True,
    ).astype(jnp.float32)
    log_mass = mass.transpose(1, 2, 0, 3)
    mixed = summed.astype(jnp.bfloat16).reshape(1, rows_dev, summed.shape[1])
    return (mixed, log_mass)


CHUNK = 128


def level_sums(length):
    levels = length.bit_length() - 1
    row = np.arange(length)
    spans = []
    for level in range(levels):
        half = 1 << level
        middle = (row // (2 * half)) * (2 * half) + half - 1
        low, high = np.minimum(row, middle), np.maximum(row, middle)
        spans.append((row[None, :] > low[:, None]) & (row[None, :] <= high[:, None]))
    spans.append(row[None, :] <= row[:, None])
    spans.append(row[None, :] > row[:, None])
    table = np.concatenate(spans, axis=0)
    return np.concatenate([table, table], axis=1).astype(np.float32)


def turn_tables(length):
    half = DIFF_HEAD // 2
    inv_freq = rope_base ** (-np.arange(half, dtype=np.float64) * (2.0 / DIFF_HEAD))
    angles = np.arange(length, dtype=np.float64)[:, None] * inv_freq[None, :]
    cos, sin = np.cos(angles), np.sin(angles)
    return (
        np.concatenate([cos, cos], axis=1).astype(np.float32),
        np.concatenate([-sin, sin], axis=1).astype(np.float32),
    )


def nt(a, b):
    return lax.dot_general(a, b, (((1,), (1,)), ((), ())), preferred_element_type=jnp.float32)


def tn(a, b):
    return lax.dot_general(a, b, (((0,), (0,)), ((), ())), preferred_element_type=jnp.float32)


def nn(a, b):
    return jnp.dot(a, b, preferred_element_type=jnp.float32)


WEIGHTS = 10


def layer_kernel(
    sizes,
    tok_ref, shift_ref, gain_ref, bias_ref, lam_ref, lgain_ref, sgain_ref, *refs,
):
    far = refs[:WEIGHTS]
    lo_far, so_far = refs[WEIGHTS : WEIGHTS + 2]
    out_ref, all_mass_ref = refs[WEIGHTS + 2 : WEIGHTS + 4]
    near = refs[WEIGHTS + 4 : 2 * WEIGHTS + 4]
    (
        wout_ref, x_ref, rows_ref, q_s, k_s, v_s, dec_s, a_s, b_s, c_s, state_s, mix_s, omix_s,
        mass_ref, via, via_shift, own_s, later_s, first_x, first_y, got_x, got_y,
        second_x, second_y, more_x, more_y, final,
        wsem, osem, wo_send, wo_recv, sc_send, via_recv, z_send, in_recv,
        sh_send, sh_recv, shz_send, shz_recv,
        g_send, g_recv, h_send, h_recv, ac_send, ac_recv, mix_send, mix_recv,
        f_send, f_recv, s_send, s_recv, home_send, home_recv, msend, mrecv,
    ) = refs[2 * WEIGHTS + 4 :]
    lq_ref, lk_ref, ld_ref, lv_ref, cos_ref, sin_ref, sq_ref, sk_ref, sv_ref, span_ref = near
    planes, count, parts, piece, width = x_ref.shape
    rows = count * piece
    half = piece // 2
    scale = DIFF_HEAD ** (-0.5)
    bf = jnp.bfloat16
    me_sp, me_fs, me_tp = lax.axis_index("sp"), lax.axis_index("fs"), lax.axis_index("tp")
    other = 1 - me_tp
    home = me_sp == me_fs
    low, high_bit = me_fs % 2, me_fs // 2
    beside = high_bit * 2 + 1 - low
    above = (1 - high_bit) * 2 + low
    across_from = (1 - high_bit) * 2 + 1 - low
    columns = (me_fs, beside, above, across_from)

    def remote(src, dst, send, recv, sp, fs, tp):
        return pltpu.make_async_remote_copy(
            src_ref=src,
            dst_ref=dst,
            send_sem=send,
            recv_sem=recv,
            device_id={"sp": sp, "fs": fs, "tp": tp},
            device_id_type=pl.DeviceIdType.MESH,
        )

    def landed(ref, sem):
        pltpu.make_async_copy(ref, ref, sem).wait()

    def piece_of(c):
        return tok_ref.at[pl.ds(pl.multiple_of(c * piece, piece), piece)]

    def rows_out(r):
        c = columns[r]
        return remote(
            piece_of(c), via.at[r - 1], sc_send.at[r - 1], via_recv.at[r - 1], me_sp, c, me_tp
        )

    def rows_home(r):
        c = columns[r]
        return remote(
            piece_of(c), x_ref.at[me_sp, c, me_tp],
            sc_send.at[r - 1], in_recv.at[me_sp], me_sp, c, me_tp,
        )

    def rows_on(r):
        src = piece_of(me_fs) if r == 0 else via.at[r - 1]
        return remote(
            src, x_ref.at[me_sp, me_fs, me_tp],
            z_send.at[r], in_recv.at[me_sp], columns[r], me_fs, me_tp,
        )

    def shift_out(r):
        return remote(
            shift_ref, via_shift.at[r - 1],
            sh_send.at[r - 1], sh_recv.at[r - 1], me_sp, columns[r], me_tp,
        )

    def shift_on(r):
        src = shift_ref if r == 0 else via_shift.at[r - 1]
        return remote(
            src, rows_ref.at[me_sp], shz_send.at[r], shz_recv.at[me_sp], columns[r], me_fs, me_tp
        )

    def near_copy(p, r):
        block = x_ref.at[p, me_fs, me_tp]
        return remote(
            block, block, g_send.at[p, r - 1], g_recv.at[p, r - 1], me_sp, columns[r], me_tp
        )

    def half_copy(p, r):
        block = x_ref.at[p, columns[3 - r], me_tp, pl.ds((r % 2) * half, half)]
        return remote(
            block, block, h_send.at[p, r - 1], h_recv.at[p, r - 1], me_sp, columns[r], me_tp
        )

    def across(p, r):
        if r < 3:
            block = x_ref.at[p, columns[r], me_tp]
        else:
            block = x_ref.at[p, columns[3], me_tp, pl.ds((r - 3) * half, half)]
        return remote(block, block, ac_send.at[p, r], ac_recv.at[p, r], me_sp, me_fs, other)

    def crossed(p, r):
        if r < 3:
            landed(x_ref.at[p, columns[r], other], ac_recv.at[p, r])
        else:
            landed(x_ref.at[p, columns[3], other, pl.ds((r - 3) * half, half)], ac_recv.at[p, r])

    def mix_out(j):
        here = pl.ds(j * rows, rows)
        return remote(
            mix_s.at[here], omix_s.at[here], mix_send.at[j], mix_recv.at[j], me_sp, me_fs, other
        )

    def first_out(j, r):
        src, dst = (first_x, got_x) if r == 1 else (first_y, got_y)
        return remote(
            src.at[j], dst.at[j], f_send.at[j, r - 1], f_recv.at[j, r - 1],
            me_sp, columns[r], me_tp,
        )

    def second_out(j, r):
        src, dst = (second_x, more_x) if r == 1 else (second_y, more_y)
        return remote(
            src.at[j], dst.at[j], s_send.at[j, r - 1], s_recv.at[j, r - 1],
            me_sp, columns[r], me_tp,
        )

    def home_out(p):
        return remote(
            final.at[p], out_ref.at[me_fs], home_send.at[p], home_recv.at[me_fs], p, me_sp, me_tp
        )

    def mass_out(p):
        return remote(
            mass_ref.at[p], all_mass_ref.at[me_sp], msend.at[p], mrecv.at[me_sp], p, me_fs, me_tp
        )

    def mine(p):
        return jnp.logical_and(home, p == me_sp)

    def own_cols(t):
        return pl.ds(pl.multiple_of(t * width, width), width)

    loads = [pltpu.make_async_copy(f, n, wsem.at[i]) for i, (f, n) in enumerate(zip(far, near))]
    depth = lo_far.shape[0]
    out_loads = [
        pltpu.make_async_copy(
            f.at[:, own_cols(me_tp)], wout_ref.at[0, pl.ds(i * depth, depth)], osem.at[i]
        )
        for i, f in enumerate((lo_far, so_far))
    ]
    out_gives = [
        remote(
            f.at[:, own_cols(other)], wout_ref.at[1, pl.ds(i * depth, depth)],
            wo_send.at[i], wo_recv.at[i], me_sp, me_fs, other,
        )
        for i, f in enumerate((lo_far, so_far))
    ]

    barrier = pltpu.get_barrier_semaphore()
    partners = [(me_sp, c, me_tp) for c in columns[1:]] + [(me_sp, me_fs, other)]
    partners += [(lax.rem(me_sp + d, planes), me_fs, me_tp) for d in range(1, planes)]
    for sp, fs, tp in partners:
        pl.semaphore_signal(
            barrier, inc=1, device_id={"sp": sp, "fs": fs, "tp": tp},
            device_id_type=pl.DeviceIdType.MESH,
        )
    for load in loads:
        load.start()
    for load in out_loads:
        load.start()
    pl.semaphore_wait(barrier, len(partners))

    @pl.when(home)
    def _():
        for r in (3, 1, 2):
            rows_home(r).start()
        pltpu.make_async_copy(
            piece_of(me_fs), x_ref.at[me_sp, me_fs, me_tp], in_recv.at[me_sp]
        ).start()
        pltpu.make_async_copy(shift_ref, rows_ref.at[me_sp], shz_recv.at[me_sp]).start()

    @pl.when(jnp.logical_not(home))
    def _():
        for r in (3, 1, 2):
            rows_out(r).start()
        rows_on(0).start()
        shift_on(0).start()

    for r in (1, 2, 3):
        shift_out(r).start()

    def forward(r):
        stay = columns[r] == me_sp

        @pl.when(jnp.logical_not(stay))
        def _():
            landed(via.at[r - 1], via_recv.at[r - 1])
            rows_on(r).start()
            landed(via_shift.at[r - 1], sh_recv.at[r - 1])
            shift_on(r).start()

        @pl.when(stay)
        def _():
            landed(via_shift.at[r - 1], sh_recv.at[r - 1])
            pltpu.make_async_copy(
                via_shift.at[r - 1], rows_ref.at[me_sp], shz_recv.at[me_sp]
            ).start()

    for r in (1, 2, 3):
        forward(r)
    for give in out_gives:
        give.start()

    def arrive(p):
        landed(x_ref.at[p, me_fs, me_tp], in_recv.at[p])
        near_copy(p, 1).start()
        near_copy(p, 2).start()
        across(p, 0).start()

    def relay(p):
        for r in (1, 2):
            landed(x_ref.at[p, columns[r], me_tp], g_recv.at[p, r - 1])
            half_copy(p, 3 - r).start()
            across(p, r).start()

    def gather_rest(p):
        for r in (1, 2):
            landed(
                x_ref.at[p, columns[3], me_tp, pl.ds((r % 2) * half, half)], h_recv.at[p, r - 1]
            )
            across(p, 3 + r % 2).start()

    def complete(p):
        for r in range(5):
            crossed(p, r)
        landed(rows_ref.at[p], shz_recv.at[p])

    def project_rows(p):
        here = pl.ds(pl.multiple_of(p * rows, rows), rows)
        halves = [x_ref[p, :, t].reshape(rows, width).astype(jnp.float32) for t in range(parts)]
        square = sum(jnp.sum(h * h, axis=-1, keepdims=True) for h in halves)
        factor = lax.rsqrt(square / (parts * width) + norm_eps)
        normed = jnp.concatenate(
            [
                (h * factor * gain_ref[:, t * width : (t + 1) * width]).astype(bf)
                for t, h in enumerate(halves)
            ],
            axis=1,
        )
        qk = nn(normed, jnp.concatenate([lq_ref[...], lk_ref[...]], axis=1)).astype(bf)
        q_s[here, :] = qk[:, :GLA_KEY]
        k_s[here, :] = qk[:, GLA_KEY:]
        v_s[here, :] = nn(normed, lv_ref[...]).astype(bf)
        lane = lax.broadcasted_iota(jnp.int32, (rows_ref.shape[1], 2 * GLA_KEY), 1)
        sub = lax.broadcasted_iota(jnp.int32, (rows_ref.shape[1], 2 * GLA_KEY), 0)
        pick = jnp.where(sub == lane // GLA_KEY, 1.0, 0.0).astype(bf)
        shift = tn(rows_ref[p], pick)
        gate = nn(normed, ld_ref[...]) + bias_ref[...] + shift[:, :GLA_KEY]
        log_sig = jnp.minimum(gate, 0.0) - jnp.log1p(jnp.exp(-jnp.abs(gate)))
        dec_s[here, :] = log_sig * (1.0 / decay_tau) + shift[:, GLA_KEY:]
        cos, sin = cos_ref[here, :], sin_ref[here, :]
        for w_ref, dst in ((sq_ref, a_s), (sk_ref, b_s)):
            wide = nn(normed, w_ref[...]).astype(bf).astype(jnp.float32)
            for m in range(2):
                one = wide[:, m * DIFF_HEAD : (m + 1) * DIFF_HEAD]
                turned = one * cos + pltpu.roll(one, DIFF_HEAD // 2, 1) * sin
                dst[here, m * DIFF_HEAD : (m + 1) * DIFF_HEAD] = turned.astype(bf)
        c_s[here, :] = nn(normed, sv_ref[...]).astype(bf)

    levels = CHUNK.bit_length() - 1
    row = lax.broadcasted_iota(jnp.int32, (CHUNK, CHUNK), 0)
    col = lax.broadcasted_iota(jnp.int32, (CHUNK, CHUNK), 1)
    apart = row ^ col

    def advance(first):
        here = pl.ds(first, CHUNK)
        query, key, value = q_s[here, :].astype(jnp.float32), k_s[here, :].astype(jnp.float32), v_s[here, :]
        decay = dec_s[here, :]
        high = decay.astype(bf)
        low = (decay - high.astype(jnp.float32)).astype(bf)
        factors = jnp.exp(nn(span_ref[...], jnp.concatenate([high, low], axis=0)))
        scores = nt(q_s[here, :], k_s[here, :])
        for level in range(levels):
            factor = factors[level * CHUNK : (level + 1) * CHUNK]
            one = nt((query * factor).astype(bf), (key * factor).astype(bf))
            scores = jnp.where((apart >> level) == 1, one, scores)
        scores = jnp.where(row >= col, scores, 0.0).astype(bf)
        gone = factors[levels * CHUNK : (levels + 1) * CHUNK]
        left = factors[(levels + 1) * CHUNK :]
        state = state_s[...]
        raw = nn(scores, value) + nt((query * gone).astype(bf), state.astype(bf))
        state_s[...] = state * gone[CHUNK - 1 :, :] + tn(value, (key * left).astype(bf))
        norm = lax.rsqrt(jnp.mean(raw * raw, axis=-1, keepdims=True) + norm_eps)
        mix_s[here, :GLA_VALUE] = (raw * norm * lgain_ref[...]).astype(bf)

    lam = lam_ref[0]
    rate = scale * float(np.log2(np.e))
    key_pos = lax.broadcasted_iota(jnp.int32, (rows, rows), 0)
    query_pos = lax.broadcasted_iota(jnp.int32, (rows, rows), 1)

    def attend_rows(j):
        here = slice(j * rows, (j + 1) * rows)
        spans = [slice(0, j * rows), here] if j else [here]
        pieces = []
        for m in range(2):
            lanes = slice(m * DIFF_HEAD, (m + 1) * DIFF_HEAD)
            scores = [nt(b_s[span, lanes], a_s[here, lanes]) for span in spans]
            scores[-1] = jnp.where(key_pos <= query_pos, scores[-1], -jnp.inf)
            top = functools.reduce(
                jnp.maximum, [jnp.max(one, axis=0, keepdims=True) for one in scores]
            )
            mass = [jnp.exp2((one - top) * rate) for one in scores]
            total = sum(jnp.sum(one, axis=0, keepdims=True) for one in mass)
            mass_ref[j, m : m + 1, :] = top * scale + jnp.log(total)
            pieces.append((mass, 1.0 / total))
        (one, one_rate), (two, two_rate) = pieces
        two_rate = lam * two_rate
        raw = sum(
            tn((u * one_rate - w * two_rate).astype(bf), c_s[span, :])
            for u, w, span in zip(one, two, spans)
        )
        norm = lax.rsqrt(jnp.mean(raw * raw, axis=-1, keepdims=True) + norm_eps)
        mix_s[here, GLA_VALUE:] = (raw * norm * sgain_ref[...]).astype(bf)

        @pl.when(j != me_sp)
        def _():
            mass_out(j).start()

        @pl.when(j == me_sp)
        def _():
            pltpu.make_async_copy(mass_ref.at[j], all_mass_ref.at[j], mrecv.at[j]).start()

    def mix_rows(j):
        for n in range(rows // CHUNK):
            advance(j * rows + n * CHUNK)
        attend_rows(j)
        mix_out(j).start()

    def leave(j):
        landed(omix_s.at[pl.ds(j * rows, rows)], mix_recv.at[j])

        def turned(ref):
            return jnp.concatenate(
                [
                    ref[pl.ds(pl.multiple_of(j * rows + c * piece, piece), piece), :]
                    for c in columns
                ],
                axis=0,
            )

        full = nn(turned(mix_s), wout_ref[0]) + nn(turned(omix_s), wout_ref[1])
        parted = [full[i * half : (i + 1) * half] for i in range(2 * count)]
        first_x[j, 0] = parted[2].astype(bf)
        first_x[j, 1] = parted[6].astype(bf)
        first_y[j, 0] = parted[5].astype(bf)
        first_y[j, 1] = parted[7].astype(bf)
        own_s[j, 0] = parted[0]
        own_s[j, 1] = parted[1]
        later_s[j, 0] = parted[3]
        later_s[j, 1] = parted[4]
        first_out(j, 1).start()
        first_out(j, 2).start()

    def pass_on(j):
        landed(got_x.at[j], f_recv.at[j, 0])
        second_y[j] = (later_s[j, 1] + got_x[j, 1].astype(jnp.float32)).astype(bf)
        second_out(j, 2).start()
        landed(got_y.at[j], f_recv.at[j, 1])
        second_x[j] = (later_s[j, 0] + got_y[j, 1].astype(jnp.float32)).astype(bf)
        second_out(j, 1).start()

    def finish(j):
        landed(more_y.at[j], s_recv.at[j, 1])
        final[j, pl.ds(0, half)] = (
            own_s[j, 0] + got_x[j, 0].astype(jnp.float32) + more_y[j].astype(jnp.float32)
        ).astype(bf)
        landed(more_x.at[j], s_recv.at[j, 0])
        final[j, pl.ds(half, half)] = (
            own_s[j, 1] + got_y[j, 0].astype(jnp.float32) + more_x[j].astype(jnp.float32)
        ).astype(bf)

        @pl.when(jnp.logical_not(mine(j)))
        def _():
            home_out(j).start()

        @pl.when(mine(j))
        def _():
            pltpu.make_async_copy(final.at[j], out_ref.at[me_fs], home_recv.at[me_fs]).start()

    def slot(i):
        if i == 0:
            return me_sp
        return i - 1 + (i - 1 >= me_sp).astype(jnp.int32)

    state_s[...] = jnp.zeros_like(state_s)
    order = [slot(i) for i in range(planes)]
    arrive(order[0])
    relay(order[0])
    arrive(order[1])
    gather_rest(order[0])
    complete(order[0])
    for load in loads:
        load.wait()
    project_rows(order[0])

    relay(order[1])
    arrive(order[2])
    gather_rest(order[1])
    complete(order[1])
    project_rows(order[1])
    mix_rows(0)

    relay(order[2])
    arrive(order[3])
    for load in out_loads:
        load.wait()
    for give in out_gives:
        give.wait_recv()
    leave(0)
    gather_rest(order[2])
    complete(order[2])
    project_rows(order[2])
    mix_rows(1)

    relay(order[3])
    leave(1)
    pass_on(0)
    gather_rest(order[3])
    complete(order[3])
    project_rows(order[3])
    mix_rows(2)
    finish(0)
    pass_on(1)
    leave(2)
    mix_rows(3)
    finish(1)
    pass_on(2)
    leave(3)
    finish(2)
    pass_on(3)
    finish(3)

    for p in range(planes):
        landed(all_mass_ref.at[p], mrecv.at[p])
        mix_out(p).wait_send()
        for r in range(5):
            across(p, r).wait_send()
        for r in (1, 2):
            near_copy(p, r).wait_send()
            half_copy(p, r).wait_send()
            first_out(p, r).wait_send()
            second_out(p, r).wait_send()

        @pl.when(p != me_sp)
        def _():
            mass_out(p).wait_send()

        @pl.when(jnp.logical_not(mine(p)))
        def _():
            home_out(p).wait_send()

    for give in out_gives:
        give.wait_send()

    @pl.when(jnp.logical_not(home))
    def _():
        rows_on(0).wait_send()
        shift_on(0).wait_send()

    for r in (1, 2, 3):
        rows_out(r).wait_send()
        shift_out(r).wait_send()

        @pl.when(columns[r] != me_sp)
        def _():
            rows_on(r).wait_send()
            shift_on(r).wait_send()

    for c in range(count):
        landed(out_ref.at[c], home_recv.at[c])


def turned_shards(
    sizes,
    tokens,
    norm_gain,
    lin_query,
    lin_key,
    lin_value,
    lin_decay,
    decay_bias,
    decay_shift,
    soft_query,
    soft_key,
    soft_value,
    soft_lambda,
    lin_gain,
    soft_gain,
    lin_out,
    soft_out,
):
    rows, width = tokens.shape[1:]
    planes, count, parts = sizes["sp"], sizes["fs"], sizes["tp"]
    piece = rows // count
    half = piece // 2
    length = planes * rows
    head = lax.axis_index("fs") * parts + lax.axis_index("tp")
    bf, f32 = jnp.bfloat16, jnp.float32
    vmem = pl.BlockSpec(memory_space=pltpu.VMEM)
    dma = pltpu.SemaphoreType.DMA
    shift = jnp.pad(decay_shift[:, 0, :], ((0, 14), (0, 0)))
    own_lambda = lax.dynamic_slice_in_dim(soft_lambda, head, 1, 0)
    own_bias = lax.dynamic_slice_in_dim(decay_bias, head * GLA_KEY, GLA_KEY, 0)[None]
    cos, sin = turn_tables(length)
    weights = (
        lin_query, lin_key, lin_decay, lin_value, jnp.asarray(cos), jnp.asarray(sin),
        soft_query, soft_key, soft_value, jnp.asarray(level_sums(CHUNK), bf),
    )
    mixed, all_mass = pl.pallas_call(
        functools.partial(layer_kernel, sizes),
        out_shape=(
            jax.ShapeDtypeStruct((count, piece, width), bf),
            jax.ShapeDtypeStruct((planes, 2, rows), f32),
        ),
        in_specs=[vmem] * 4
        + [pl.BlockSpec(memory_space=pltpu.SMEM)]
        + [vmem] * 2
        + [pl.BlockSpec(memory_space=pl.ANY)] * (WEIGHTS + 2),
        out_specs=[vmem] * 2,
        scratch_shapes=[pltpu.VMEM(w.shape, w.dtype) for w in weights]
        + [
            pltpu.VMEM((2, GLA_VALUE + DIFF_VALUE, width), bf),
            pltpu.VMEM((planes, count, parts, piece, width), bf),
            pltpu.VMEM((planes, 16, rows), bf),
            pltpu.VMEM((length, GLA_KEY), bf),
            pltpu.VMEM((length, GLA_KEY), bf),
            pltpu.VMEM((length, GLA_VALUE), bf),
            pltpu.VMEM((length, GLA_KEY), f32),
            pltpu.VMEM((length, 2 * DIFF_HEAD), bf),
            pltpu.VMEM((length, 2 * DIFF_HEAD), bf),
            pltpu.VMEM((length, DIFF_VALUE), bf),
            pltpu.VMEM((GLA_VALUE, GLA_KEY), f32),
            pltpu.VMEM((length, GLA_VALUE + DIFF_VALUE), bf),
            pltpu.VMEM((length, GLA_VALUE + DIFF_VALUE), bf),
            pltpu.VMEM((planes, 2, rows), f32),
            pltpu.VMEM((count - 1, piece, width), bf),
            pltpu.VMEM((count - 1, 16, rows), bf),
            pltpu.VMEM((planes, 2, half, width), f32),
            pltpu.VMEM((planes, 2, half, width), f32),
            pltpu.VMEM((planes, 2, half, width), bf),
            pltpu.VMEM((planes, 2, half, width), bf),
            pltpu.VMEM((planes, 2, half, width), bf),
            pltpu.VMEM((planes, 2, half, width), bf),
            pltpu.VMEM((planes, half, width), bf),
            pltpu.VMEM((planes, half, width), bf),
            pltpu.VMEM((planes, half, width), bf),
            pltpu.VMEM((planes, half, width), bf),
            pltpu.VMEM((planes, piece, width), bf),
            dma((WEIGHTS,)), dma((2,)), dma((2,)), dma((2,)),
            dma((count - 1,)), dma((count - 1,)), dma((count,)), dma((planes,)),
            dma((count - 1,)), dma((count - 1,)), dma((count,)), dma((planes,)),
            dma((planes, 2)), dma((planes, 2)), dma((planes, 2)), dma((planes, 2)),
            dma((planes, 5)), dma((planes, 5)), dma((planes,)), dma((planes,)),
            dma((planes, 2)), dma((planes, 2)), dma((planes, 2)), dma((planes, 2)),
            dma((planes,)), dma((count,)), dma((planes,)), dma((planes,)),
        ],
        compiler_params=pltpu.CompilerParams(
            has_side_effects=True, collective_id=0, vmem_limit_bytes=60 * 1024 * 1024
        ),
        name="whole_layer",
    )(
        tokens[0], shift, norm_gain[None], own_bias, own_lambda, lin_gain[None], soft_gain[None],
        *weights, lin_out, soft_out,
    )
    return mixed.reshape(1, rows, width), all_mass.transpose(1, 0, 2)[None]


def solution(mesh):
    in_specs = (
        P("fs", "sp", "tp"),
        P(),
        P(None, ("fs", "tp")),
        P(None, ("fs", "tp")),
        P(None, ("fs", "tp")),
        P(None, ("fs", "tp")),
        P(),
        P(None, "fs", "sp"),
        P(None, ("fs", "tp")),
        P(None, ("fs", "tp")),
        P(None, ("fs", "tp")),
        P(),
        P(),
        P(),
        P(("fs", "tp"), None),
        P(("fs", "tp"), None),
    )
    out_specs = (P("fs", "sp", "tp"), P(("fs", "tp"), None, None, "sp"))
    sizes = dict(mesh.shape)

    def per_device(*args):
        one_head = args[2].shape[1] == GLA_KEY and args[10].shape[1] == DIFF_VALUE
        square = sizes["fs"] == sizes["sp"] == 4 and sizes["tp"] == 2 and args[0].shape[0] == 1
        if one_head and square:
            return turned_shards(sizes, *args)
        return shards(*args)

    return jax.shard_map(per_device, mesh=mesh, in_specs=in_specs, out_specs=out_specs, check_vma=False)
```

```python
import functools

import jax
import jax.numpy as jnp
import numpy as np
from jax import lax
from jax.experimental import pallas as pl
from jax.experimental.pallas import tpu as pltpu
from jax.sharding import PartitionSpec as P

GLA_KEY = 128
GLA_VALUE = 256
DIFF_HEAD = 128
DIFF_VALUE = 256
BLOCK = 64


norm_eps = 1e-06
decay_tau = 16.0
rope_base = 500000.0
highest = lax.Precision.HIGHEST


def prefix(array, axis, join, neutral):
    place = lax.axis_index(axis)
    gathered = jax.tree.map(
        lambda a, kind: lax.all_gather(a.astype(kind), axis), array, (jnp.bfloat16, jnp.bfloat16)
    )
    state = jax.tree.map(lambda a, e: jnp.zeros_like(a) + jnp.asarray(e, a.dtype), array, neutral)

    def one(turn, state):
        return join(
            state,
            jax.tree.map(
                lambda a, own: lax.dynamic_index_in_dim(a, turn, 0, False).astype(own.dtype),
                gathered,
                array,
            ),
        )

    return lax.fori_loop(0, place, one, state)


def scaled_rms(values, norm_gain):
    return (
        values * lax.rsqrt(jnp.mean(values * values, axis=-1, keepdims=True) + norm_eps) * norm_gain
    )


def rotate(values, positions):
    half_dim = values.shape[-1] // 2
    inv_freq = jnp.power(
        jnp.float32(rope_base), -jnp.arange(half_dim, dtype=jnp.float32) * (2.0 / values.shape[-1])
    )
    angles = positions.astype(jnp.float32)[:, None] * inv_freq[None, :]
    cos_table = jnp.cos(angles)[:, None, None, :]
    sin_table = jnp.sin(angles)[:, None, None, :]
    widened = values.astype(jnp.float32)
    first_half = widened[..., :half_dim]
    second_half = widened[..., half_dim:]
    turned = jnp.concatenate(
        [
            first_half * cos_table - second_half * sin_table,
            second_half * cos_table + first_half * sin_table,
        ],
        axis=-1,
    )
    return turned.astype(jnp.bfloat16)


def block_pass(queries, key_rows, value_rows, log_decay, block_len):
    groups, length, heads, key_dim = queries.shape
    value_dim = value_rows.shape[-1]
    block_count = length // block_len

    def split(tensor):
        return tensor.reshape(groups, block_count, block_len, heads, tensor.shape[-1]).transpose(
            1, 0, 3, 2, 4
        )

    causal = jnp.tril(jnp.ones((block_len, block_len), dtype=bool))[:, :, None]

    def advance(carry, inputs):
        state_now, offset = carry
        query_blk, key_blk, value_blk, decay_blk = inputs
        cum_log = jnp.cumsum(decay_blk, axis=2)
        inner_part = jnp.einsum(
            "bhcd,bhdv->bhcv", query_blk * jnp.exp(cum_log), state_now, precision=highest
        )
        decay_pair = jnp.exp(
            jnp.where(causal, cum_log[:, :, :, None, :] - cum_log[:, :, None, :, :], -jnp.inf)
        )
        scores = jnp.sum(
            query_blk[:, :, :, None, :] * key_blk[:, :, None, :, :] * decay_pair, axis=-1
        )
        local_part = jnp.einsum("bhij,bhjv->bhiv", scores, value_blk, precision=highest)
        last_log = cum_log[:, :, -1, :]
        state_now = jnp.exp(last_log)[..., None] * state_now + jnp.einsum(
            "bhcd,bhcv->bhdv",
            key_blk * jnp.exp(last_log[:, :, None, :] - cum_log),
            value_blk,
            precision=highest,
        )
        carried = query_blk * jnp.exp(offset[:, :, None, :] + cum_log)
        return ((state_now, offset + last_log), (inner_part + local_part, carried))

    start = (
        jnp.zeros((groups, heads, key_dim, value_dim), jnp.float32),
        jnp.zeros((groups, heads, key_dim), jnp.float32),
    )
    (state_end, offset_end), (outs, carried) = lax.scan(
        advance, start, (split(queries), split(key_rows), split(value_rows), split(log_decay))
    )
    return (outs, carried, state_end, offset_end)


def project(rows, weight):
    lead_shape = rows.shape[:-1]
    flat_rows = rows.reshape(-1, rows.shape[-1])
    product = jnp.dot(flat_rows, weight, preferred_element_type=jnp.float32)
    return product.reshape(lead_shape + (weight.shape[1],))


def chain_join(earlier, later):
    return (earlier[0] * later[0], later[0][..., None] * earlier[1] + later[1])


def attend(queries, query_pos, reach, all_keys, all_values, soft_lambda, soft_gain, rows_dev):
    groups, query_rows, soft_heads = queries.shape[:3]
    block_total = all_keys.shape[1] // rows_dev
    scale = DIFF_HEAD ** (-0.5)

    def first_pass(block_id, carry):
        top_now, total_now, score_store = carry
        key_blk = lax.dynamic_slice_in_dim(all_keys, block_id * rows_dev, rows_dev, 1)
        raw_scores = (
            jnp.einsum("bqhmd,bkhmd->bhmqk", queries, key_blk, preferred_element_type=jnp.float32)
            * scale
        )
        key_pos = block_id * rows_dev + jnp.arange(rows_dev, dtype=jnp.int32)
        scores = jnp.where(key_pos[None, :] <= query_pos[:, None], raw_scores, -jnp.inf)
        top_next = jnp.maximum(top_now, jnp.max(scores, axis=-1))
        total_next = total_now * jnp.exp(top_now - top_next) + jnp.sum(
            jnp.exp(scores - top_next[..., None]), axis=-1
        )
        score_store = lax.dynamic_update_index_in_dim(score_store, scores, block_id, 0)
        return (top_next, total_next, score_store)

    stat_shape = (groups, soft_heads, 2, query_rows)
    store_init = jnp.full((block_total,) + stat_shape + (rows_dev,), -jnp.inf, jnp.float32)
    top_all, total_all, score_store = lax.fori_loop(
        0,
        reach,
        first_pass,
        (
            jnp.full(stat_shape, -jnp.inf, jnp.float32),
            jnp.zeros(stat_shape, jnp.float32),
            store_init,
        ),
    )
    mass = top_all + jnp.log(total_all)

    def second_pass(block_id, accum):
        scores = lax.dynamic_index_in_dim(score_store, block_id, 0, keepdims=False)
        probs = jnp.exp(scores - top_all[..., None]) / total_all[..., None]
        weights = (probs[:, :, 0] - soft_lambda[None, :, None, None] * probs[:, :, 1]).astype(
            jnp.bfloat16
        )
        value_blk = lax.dynamic_slice_in_dim(all_values, block_id * rows_dev, rows_dev, 1)
        return accum + jnp.einsum(
            "bhqk,bkhv->bhqv", weights, value_blk, preferred_element_type=jnp.float32
        )

    accum = lax.fori_loop(
        0, reach, second_pass, jnp.zeros((groups, soft_heads, query_rows, DIFF_VALUE), jnp.float32)
    )
    soft_mix = scaled_rms(accum, soft_gain).astype(jnp.bfloat16).transpose(0, 2, 1, 3)
    soft_mix = soft_mix.reshape(groups, query_rows, soft_heads * DIFF_VALUE)
    return (soft_mix, mass)


def mixers(
    normed,
    shift_rows,
    lin_query,
    lin_key,
    lin_value,
    lin_decay,
    decay_bias,
    soft_query,
    soft_key,
    soft_value,
    soft_lambda,
    lin_gain,
    soft_gain,
):
    groups, rows_dev, model_width = normed.shape
    lin_heads = lin_query.shape[1] // GLA_KEY
    soft_heads = soft_value.shape[1] // DIFF_VALUE
    place = lax.axis_index("sp")
    shift_wide = shift_rows.astype(jnp.float32)
    lin_q = (
        project(normed, lin_query)
        .astype(jnp.bfloat16)
        .reshape(groups, rows_dev, lin_heads, GLA_KEY)
    )
    lin_k = (
        project(normed, lin_key).astype(jnp.bfloat16).reshape(groups, rows_dev, lin_heads, GLA_KEY)
    )
    lin_v = (
        project(normed, lin_value)
        .astype(jnp.bfloat16)
        .reshape(groups, rows_dev, lin_heads, GLA_VALUE)
    )
    gate_input = project(normed, lin_decay) + decay_bias + shift_wide[0][:, :, None]
    log_decay = jax.nn.log_sigmoid(gate_input) / decay_tau + shift_wide[1][:, :, None]
    log_decay = log_decay.reshape(groups, rows_dev, lin_heads, GLA_KEY)
    outs, carried, state_end, offset_end = block_pass(
        lin_q.astype(jnp.float32),
        lin_k.astype(jnp.float32),
        lin_v.astype(jnp.float32),
        log_decay,
        BLOCK,
    )
    keep_in, state_in = prefix(
        (jnp.exp(offset_end), state_end),
        "sp",
        chain_join,
        (jnp.ones_like(offset_end), jnp.zeros_like(state_end)),
    )
    outs = outs + jnp.einsum("nbhcd,bhdv->nbhcv", carried, state_in, precision=highest)
    lin_raw = outs.transpose(1, 0, 3, 2, 4).reshape(groups, rows_dev, lin_heads, GLA_VALUE)
    lin_mix = (
        scaled_rms(lin_raw, lin_gain)
        .astype(jnp.bfloat16)
        .reshape(groups, rows_dev, lin_heads * GLA_VALUE)
    )
    positions = place * rows_dev + jnp.arange(rows_dev, dtype=jnp.int32)
    soft_q = rotate(
        project(normed, soft_query)
        .astype(jnp.bfloat16)
        .reshape(groups, rows_dev, soft_heads, 2, DIFF_HEAD),
        positions,
    )
    soft_k = rotate(
        project(normed, soft_key)
        .astype(jnp.bfloat16)
        .reshape(groups, rows_dev, soft_heads, 2, DIFF_HEAD),
        positions,
    )
    soft_v = (
        project(normed, soft_value)
        .astype(jnp.bfloat16)
        .reshape(groups, rows_dev, soft_heads, DIFF_VALUE)
    )
    all_keys, all_values = (
        lax.all_gather(soft_k, "sp", axis=1, tiled=True),
        lax.all_gather(soft_v, "sp", axis=1, tiled=True),
    )
    soft_mix, mass = attend(
        soft_q, positions, place + 1, all_keys, all_values, soft_lambda, soft_gain, rows_dev
    )
    return (lin_mix, soft_mix, mass)


def output_term(lin_mix, soft_mix, lin_out, soft_out, rows_dev, parts):
    col_width = lin_out.shape[1] // parts

    def term(start, row_count):
        pieces = []
        for turn_index in range(row_count // rows_dev):
            piece_id = (start + turn_index * rows_dev) // rows_dev
            seq_id = piece_id // parts
            part_id = piece_id % parts
            lin_rows = lax.dynamic_index_in_dim(lin_mix, seq_id, 0, keepdims=False)
            soft_rows = lax.dynamic_index_in_dim(soft_mix, seq_id, 0, keepdims=False)
            lin_cols = lax.dynamic_slice_in_dim(lin_out, part_id * col_width, col_width, 1)
            soft_cols = lax.dynamic_slice_in_dim(soft_out, part_id * col_width, col_width, 1)
            pieces.append(
                jnp.dot(lin_rows, lin_cols, preferred_element_type=jnp.float32)
                + jnp.dot(soft_rows, soft_cols, preferred_element_type=jnp.float32)
            )
        return jnp.concatenate(pieces, axis=0)

    return term


def shards(
    tokens,
    norm_gain,
    lin_query,
    lin_key,
    lin_value,
    lin_decay,
    decay_bias,
    decay_shift,
    soft_query,
    soft_key,
    soft_value,
    soft_lambda,
    lin_gain,
    soft_gain,
    lin_out,
    soft_out,
):
    rows_dev = tokens.shape[1]
    parts = lax.axis_size("tp")
    fs_size = lax.axis_size("fs")
    fs_index = lax.axis_index("fs")
    tp_index = lax.axis_index("tp")
    whole = lax.all_gather(tokens, "tp", axis=2, tiled=True).astype(jnp.float32)
    normed = scaled_rms(whole, norm_gain).astype(jnp.bfloat16)
    lambda_grid = soft_lambda.reshape(fs_size, parts, -1)
    bias_grid = decay_bias.reshape(fs_size, parts, -1)
    all_rows, all_shift = (
        lax.all_gather(normed, "fs", axis=0, tiled=True),
        lax.all_gather(decay_shift, "fs", axis=1, tiled=True),
    )
    head_lambda = lax.dynamic_index_in_dim(
        lax.dynamic_index_in_dim(lambda_grid, fs_index, 0, keepdims=False),
        tp_index,
        0,
        keepdims=False,
    )
    head_bias = lax.dynamic_index_in_dim(
        lax.dynamic_index_in_dim(bias_grid, fs_index, 0, keepdims=False),
        tp_index,
        0,
        keepdims=False,
    )
    lin_mix, soft_mix, mass = mixers(
        all_rows,
        all_shift,
        lin_query,
        lin_key,
        lin_value,
        lin_decay,
        head_bias,
        soft_query,
        soft_key,
        soft_value,
        head_lambda,
        lin_gain,
        soft_gain,
    )
    term = output_term(lin_mix, soft_mix, lin_out, soft_out, rows_dev, parts)
    summed = lax.psum_scatter(
        term(jnp.int32(0), rows_dev * lax.axis_size(("fs", "tp"))).astype(jnp.bfloat16),
        ("fs", "tp"),
        scatter_dimension=0,
        tiled=True,
    ).astype(jnp.float32)
    log_mass = mass.transpose(1, 2, 0, 3)
    mixed = summed.astype(jnp.bfloat16).reshape(1, rows_dev, summed.shape[1])
    return (mixed, log_mass)


CHUNK = 128


def level_sums(length):
    levels = length.bit_length() - 1
    row = np.arange(length)
    spans = []
    for level in range(levels):
        half = 1 << level
        middle = (row // (2 * half)) * (2 * half) + half - 1
        low, high = np.minimum(row, middle), np.maximum(row, middle)
        spans.append((row[None, :] > low[:, None]) & (row[None, :] <= high[:, None]))
    spans.append(row[None, :] <= row[:, None])
    spans.append(row[None, :] > row[:, None])
    table = np.concatenate(spans, axis=0)
    return np.concatenate([table, table], axis=1).astype(np.float32)


def turn_tables(length):
    half = DIFF_HEAD // 2
    inv_freq = rope_base ** (-np.arange(half, dtype=np.float64) * (2.0 / DIFF_HEAD))
    angles = np.arange(length, dtype=np.float64)[:, None] * inv_freq[None, :]
    cos, sin = np.cos(angles), np.sin(angles)
    return (
        np.concatenate([cos, cos], axis=1).astype(np.float32),
        np.concatenate([-sin, sin], axis=1).astype(np.float32),
    )


def nt(a, b):
    return lax.dot_general(a, b, (((1,), (1,)), ((), ())), preferred_element_type=jnp.float32)


def tn(a, b):
    return lax.dot_general(a, b, (((0,), (0,)), ((), ())), preferred_element_type=jnp.float32)


def nn(a, b):
    return jnp.dot(a, b, preferred_element_type=jnp.float32)


WEIGHTS = 17


def layer_kernel(
    sizes,
    *refs,
):
    far = refs[:WEIGHTS]
    lo_far, so_far = refs[WEIGHTS : WEIGHTS + 2]
    out_ref, all_mass_ref = refs[WEIGHTS + 2 : WEIGHTS + 4]
    near = refs[WEIGHTS + 4 : 2 * WEIGHTS + 4]
    (
        wout_ref, x_ref, rows_ref, normed_s, q_s, k_s, v_s, dec_s, a_s, b_s, c_s, state_s, mix_s, omix_s,
        mass_ref, mass_in, via, via_shift, own_s, later_s, first_x, first_y, got_x, got_y,
        second_x, second_y, more_x, more_y, final,
        wsem, osem, wo_send, wo_recv, sc_send, via_recv, z_send, in_recv,
        sh_send, sh_recv, shz_send, shz_recv,
        g_send, g_recv, h_send, h_recv, ac_send, ac_recv, mix_send, mix_recv,
        f_send, f_recv, s_send, s_recv, home_send, home_recv, msend, mrecv,
    ) = refs[2 * WEIGHTS + 4 :]
    (
        tok_ref, shift_ref, gain_ref, bias_ref, lam_ref, lgain_ref, sgain_ref,
        lq_ref, lk_ref, ld_ref, lv_ref, cos_ref, sin_ref, sq_ref, sk_ref, sv_ref, span_ref,
    ) = near
    planes, count, parts, piece, width = x_ref.shape
    rows = count * piece
    half, quarter = piece // 2, piece // 4
    scale = DIFF_HEAD ** (-0.5)
    bf = jnp.bfloat16
    me_sp, me_fs, me_tp = lax.axis_index("sp"), lax.axis_index("fs"), lax.axis_index("tp")
    other = 1 - me_tp
    home = me_sp == me_fs
    low, high_bit = me_fs % 2, me_fs // 2
    beside = high_bit * 2 + 1 - low
    above = (1 - high_bit) * 2 + low
    across_from = (1 - high_bit) * 2 + 1 - low
    columns = (me_fs, beside, above, across_from)

    def remote(src, dst, send, recv, sp, fs, tp):
        return pltpu.make_async_remote_copy(
            src_ref=src,
            dst_ref=dst,
            send_sem=send,
            recv_sem=recv,
            device_id={"sp": sp, "fs": fs, "tp": tp},
            device_id_type=pl.DeviceIdType.MESH,
        )

    def landed(ref, sem):
        pltpu.make_async_copy(ref, ref, sem).wait()

    def piece_of(c, h=0, count_of=2):
        return tok_ref.at[pl.ds(pl.multiple_of(c * piece + h * half, half), count_of * half)]

    def rows_out(r, h):
        return remote(
            piece_of(columns[r], h, 1), via.at[r - 1, h],
            sc_send.at[r - 1, h], via_recv.at[r - 1, h], me_sp, columns[r], me_tp,
        )

    def rows_home(r, h):
        c = columns[r]
        return remote(
            piece_of(c, h, 1), x_ref.at[me_sp, c, me_tp, pl.ds(h * half, half)],
            sc_send.at[r - 1, h], in_recv.at[me_sp, h], me_sp, c, me_tp,
        )

    def rows_on(r, h):
        src = piece_of(me_fs, h, 1) if r == 0 else via.at[r - 1, h]
        return remote(
            src, x_ref.at[me_sp, me_fs, me_tp, pl.ds(h * half, half)],
            z_send.at[r, h], in_recv.at[me_sp, h], columns[r], me_fs, me_tp,
        )

    def shift_out(r):
        return remote(
            shift_ref, via_shift.at[r - 1],
            sh_send.at[r - 1], sh_recv.at[r - 1], me_sp, columns[r], me_tp,
        )

    def shift_on(r):
        src = shift_ref if r == 0 else via_shift.at[r - 1]
        return remote(
            src, rows_ref.at[me_sp], shz_send.at[r], shz_recv.at[me_sp], columns[r], me_fs, me_tp
        )

    def half_of(p, c, h):
        return x_ref.at[p, c, me_tp, pl.ds(h * half, half)]

    def near_copy(p, r, k):
        block = half_of(p, me_fs, (r - 1 + k) % 2)
        return remote(
            block, block, g_send.at[p, r - 1, k], g_recv.at[p, r - 1, k],
            me_sp, columns[r], me_tp,
        )

    def half_copy(p, r):
        block = x_ref.at[p, columns[3 - r], me_tp, pl.ds((r % 2) * half, half)]
        return remote(
            block, block, h_send.at[p, r - 1], h_recv.at[p, r - 1], me_sp, columns[r], me_tp
        )

    def across(p, r):
        if r < 3:
            block = x_ref.at[p, columns[r], me_tp]
        else:
            block = x_ref.at[p, columns[3], me_tp, pl.ds((r - 3) * half, half)]
        return remote(block, block, ac_send.at[p, r], ac_recv.at[p, r], me_sp, me_fs, other)

    def crossed(p, r):
        if r < 3:
            landed(x_ref.at[p, columns[r], other], ac_recv.at[p, r])
        else:
            landed(x_ref.at[p, columns[3], other, pl.ds((r - 3) * half, half)], ac_recv.at[p, r])

    def block_rows(j):
        return pl.ds(pl.multiple_of(j * rows, rows), rows)

    def mix_out(j):
        here = block_rows(j)
        return remote(
            mix_s.at[here], omix_s.at[here], mix_send.at[j], mix_recv.at[j], me_sp, me_fs, other
        )

    def first_out(j, u, r):
        src, dst = (first_x, got_x) if r == 1 else (first_y, got_y)
        return remote(
            src.at[j, u], dst.at[j, u], f_send.at[j, u, r - 1], f_recv.at[j, u, r - 1],
            me_sp, columns[r], me_tp,
        )

    def second_out(j, u, r):
        src, dst = (second_x, more_x) if r == 1 else (second_y, more_y)
        return remote(
            src.at[j, u], dst.at[j, u], s_send.at[j, u, r - 1], s_recv.at[j, u, r - 1],
            me_sp, columns[r], me_tp,
        )

    def final_rows(p, u):
        return final.at[p, pl.ds(u * half, half)]

    def out_rows(c, u):
        return out_ref.at[c, pl.ds(u * half, half)]

    def home_out(p, u):
        return remote(
            final_rows(p, u), out_rows(me_fs, u),
            home_send.at[p, u], home_recv.at[me_fs, u], p, me_sp, me_tp,
        )

    def mass_out(p):
        return remote(
            mass_ref.at[p], mass_in.at[me_sp], msend.at[p], mrecv.at[me_sp], p, me_fs, me_tp
        )

    def mine(p):
        return jnp.logical_and(home, p == me_sp)

    def own_cols(t):
        return pl.ds(pl.multiple_of(t * width, width), width)

    loads = [pltpu.make_async_copy(f, n, wsem.at[i]) for i, (f, n) in enumerate(zip(far, near))]
    depth = lo_far.shape[0]
    out_loads = [
        pltpu.make_async_copy(
            f.at[:, own_cols(me_tp)], wout_ref.at[0, pl.ds(i * depth, depth)], osem.at[i]
        )
        for i, f in enumerate((lo_far, so_far))
    ]
    out_gives = [
        remote(
            f.at[:, own_cols(other)], wout_ref.at[1, pl.ds(i * depth, depth)],
            wo_send.at[i], wo_recv.at[i], me_sp, me_fs, other,
        )
        for i, f in enumerate((lo_far, so_far))
    ]

    barrier = pltpu.get_barrier_semaphore()
    partners = [(me_sp, c, me_tp) for c in columns[1:]] + [(me_sp, me_fs, other)]
    partners += [(lax.rem(me_sp + d, planes), me_fs, me_tp) for d in range(1, planes)]
    for sp, fs, tp in partners:
        pl.semaphore_signal(
            barrier, inc=1, device_id={"sp": sp, "fs": fs, "tp": tp},
            device_id_type=pl.DeviceIdType.MESH,
        )
    for load in loads + out_loads:
        load.start()
    for load in loads[:2]:
        load.wait()
    pl.semaphore_wait(barrier, len(partners))

    @pl.when(home)
    def _():
        for h in range(2):
            for r in (1, 2, 3):
                rows_home(r, h).start()
            pltpu.make_async_copy(
                piece_of(me_fs, h, 1), half_of(me_sp, me_fs, h), in_recv.at[me_sp, h]
            ).start()
        pltpu.make_async_copy(shift_ref, rows_ref.at[me_sp], shz_recv.at[me_sp]).start()

    @pl.when(jnp.logical_not(home))
    def _():
        for h in range(2):
            for r in (1, 2, 3):
                rows_out(r, h).start()
        shift_on(0).start()

    for r in (1, 2, 3):
        shift_out(r).start()

    def goes_at(r, stage):
        target = columns[r]
        place = me_sp + (me_sp < target).astype(jnp.int32)
        return jnp.logical_and(target != me_sp, place == stage)

    def forward_rows(stage):
        @pl.when(goes_at(0, stage))
        def _():
            for h in range(2):
                rows_on(0, h).start()

        for h in range(2):
            for r in (1, 2, 3):

                @pl.when(goes_at(r, stage))
                def _():
                    landed(via.at[r - 1, h], via_recv.at[r - 1, h])
                    rows_on(r, h).start()

    def forward_shift(r):
        landed(via_shift.at[r - 1], sh_recv.at[r - 1])

        @pl.when(columns[r] != me_sp)
        def _():
            shift_on(r).start()

        @pl.when(columns[r] == me_sp)
        def _():
            pltpu.make_async_copy(
                via_shift.at[r - 1], rows_ref.at[me_sp], shz_recv.at[me_sp]
            ).start()

    def forward_small():
        for r in (1, 2, 3):
            forward_shift(r)
        for give in out_gives:
            give.start()

    def arrive(p):
        for h in range(2):
            landed(half_of(p, me_fs, h), in_recv.at[p, h])
        for k in range(2):
            near_copy(p, 1, k).start()
            near_copy(p, 2, k).start()
        across(p, 0).start()

    def relay(p, r):
        landed(half_of(p, columns[r], r - 1), g_recv.at[p, r - 1, 0])
        half_copy(p, 3 - r).start()

    def pass_across(p, r):
        landed(half_of(p, columns[r], r % 2), g_recv.at[p, r - 1, 1])
        across(p, r).start()

    def pass_half(p, r):
        landed(half_of(p, columns[3], r % 2), h_recv.at[p, r - 1])
        across(p, 3 + r % 2).start()

    def complete(p):
        for r in range(5):
            crossed(p, r)
        landed(rows_ref.at[p], shz_recv.at[p])

    head = me_fs * parts + me_tp

    def project_rows(p):
        bias = bias_ref[:, pl.ds(pl.multiple_of(head * GLA_KEY, GLA_KEY), GLA_KEY)]
        here = pl.ds(pl.multiple_of(p * rows, rows), rows)
        halves = [x_ref[p, :, t].reshape(rows, width).astype(jnp.float32) for t in range(parts)]
        square = sum(jnp.sum(h * h, axis=-1, keepdims=True) for h in halves)
        factor = lax.rsqrt(square / (parts * width) + norm_eps)
        normed = jnp.concatenate(
            [
                (h * factor * gain_ref[:, t * width : (t + 1) * width]).astype(bf)
                for t, h in enumerate(halves)
            ],
            axis=1,
        )
        normed_s[...] = normed
        qk = nn(normed, jnp.concatenate([lq_ref[...], lk_ref[...]], axis=1)).astype(bf)
        q_s[here, :] = qk[:, :GLA_KEY]
        k_s[here, :] = qk[:, GLA_KEY:]
        v_s[here, :] = nn(normed, lv_ref[...]).astype(bf)
        lane = lax.broadcasted_iota(jnp.int32, (rows_ref.shape[1], 2 * GLA_KEY), 1)
        sub = lax.broadcasted_iota(jnp.int32, (rows_ref.shape[1], 2 * GLA_KEY), 0)
        pick = jnp.where(sub == lane // GLA_KEY, 1.0, 0.0).astype(bf)
        shift = tn(rows_ref[p], pick)
        gate = nn(normed, ld_ref[...]) + bias + shift[:, :GLA_KEY]
        log_sig = jnp.minimum(gate, 0.0) - jnp.log1p(jnp.exp(-jnp.abs(gate)))
        dec_s[here, :] = log_sig * (1.0 / decay_tau) + shift[:, GLA_KEY:]

    def project_soft(p):
        here = pl.ds(pl.multiple_of(p * rows, rows), rows)
        normed = normed_s[...]
        cos, sin = cos_ref[here, :], sin_ref[here, :]
        for w_ref, dst in ((sq_ref, a_s), (sk_ref, b_s)):
            wide = nn(normed, w_ref[...]).astype(bf).astype(jnp.float32)
            for m in range(2):
                one = wide[:, m * DIFF_HEAD : (m + 1) * DIFF_HEAD]
                turned = one * cos + pltpu.roll(one, DIFF_HEAD // 2, 1) * sin
                dst[here, m * DIFF_HEAD : (m + 1) * DIFF_HEAD] = turned.astype(bf)
        c_s[here, :] = nn(normed, sv_ref[...]).astype(bf)

    levels = CHUNK.bit_length() - 1
    row = lax.broadcasted_iota(jnp.int32, (CHUNK, CHUNK), 0)
    col = lax.broadcasted_iota(jnp.int32, (CHUNK, CHUNK), 1)
    apart = row ^ col

    def advance(first):
        here = pl.ds(first, CHUNK)
        query, key, value = q_s[here, :].astype(jnp.float32), k_s[here, :].astype(jnp.float32), v_s[here, :]
        decay = dec_s[here, :]
        high = decay.astype(bf)
        low = (decay - high.astype(jnp.float32)).astype(bf)
        factors = jnp.exp(nn(span_ref[...], jnp.concatenate([high, low], axis=0)))
        scores = nt(q_s[here, :], k_s[here, :])
        for level in range(levels):
            factor = factors[level * CHUNK : (level + 1) * CHUNK]
            one = nt((query * factor).astype(bf), (key * factor).astype(bf))
            scores = jnp.where((apart >> level) == 1, one, scores)
        scores = jnp.where(row >= col, scores, 0.0).astype(bf)
        gone = factors[levels * CHUNK : (levels + 1) * CHUNK]
        left = factors[(levels + 1) * CHUNK :]
        state = state_s[...]
        raw = nn(scores, value) + nt((query * gone).astype(bf), state.astype(bf))
        state_s[...] = state * gone[CHUNK - 1 :, :] + tn(value, (key * left).astype(bf))
        norm = lax.rsqrt(jnp.mean(raw * raw, axis=-1, keepdims=True) + norm_eps)
        mix_s[here, :GLA_VALUE] = (raw * norm * lgain_ref[...]).astype(bf)

    heads_at = lax.broadcasted_iota(jnp.int32, lam_ref.shape, 1)
    rate = scale * float(np.log2(np.e))
    key_pos = lax.broadcasted_iota(jnp.int32, (rows, rows), 0)
    query_pos = lax.broadcasted_iota(jnp.int32, (rows, rows), 1)

    def attend_rows(j):
        here = slice(j * rows, (j + 1) * rows)
        spans = [slice(0, j * rows), here] if j else [here]
        pieces = []
        for m in range(2):
            lanes = slice(m * DIFF_HEAD, (m + 1) * DIFF_HEAD)
            scores = [nt(b_s[span, lanes], a_s[here, lanes]) for span in spans]
            scores[-1] = jnp.where(key_pos <= query_pos, scores[-1], -jnp.inf)
            top = functools.reduce(
                jnp.maximum, [jnp.max(one, axis=0, keepdims=True) for one in scores]
            )
            mass = [jnp.exp2((one - top) * rate) for one in scores]
            total = sum(jnp.sum(one, axis=0, keepdims=True) for one in mass)
            mass_ref[j, m : m + 1, :] = top * scale + jnp.log(total)
            pieces.append((mass, 1.0 / total))
        (one, one_rate), (two, two_rate) = pieces
        lam = jnp.sum(jnp.where(heads_at == head, lam_ref[...], 0.0), axis=1, keepdims=True)
        two_rate = lam * two_rate
        raw = sum(
            tn((u * one_rate - w * two_rate).astype(bf), c_s[span, :])
            for u, w, span in zip(one, two, spans)
        )
        norm = lax.rsqrt(jnp.mean(raw * raw, axis=-1, keepdims=True) + norm_eps)
        mix_s[here, GLA_VALUE:] = (raw * norm * sgain_ref[...]).astype(bf)

        @pl.when(j != me_sp)
        def _():
            mass_out(j).start()

        @pl.when(j == me_sp)
        def _():
            pltpu.make_async_copy(mass_ref.at[j], mass_in.at[j], mrecv.at[j]).start()

    def advance_rows(j):
        for n in range(rows // CHUNK):
            advance(j * rows + n * CHUNK)

    def leave(j, u):
        if u == 0:
            landed(omix_s.at[block_rows(j)], mix_recv.at[j])

        def turned(ref):
            starts = [pl.multiple_of(j * rows + c * piece + u * half, half) for c in columns]
            return jnp.concatenate([ref[pl.ds(start, half), :] for start in starts], axis=0)

        full = nn(turned(mix_s), wout_ref[0]) + nn(turned(omix_s), wout_ref[1])
        parted = [full[i * quarter : (i + 1) * quarter] for i in range(2 * count)]
        first_x[j, u, 0] = parted[2].astype(bf)
        first_x[j, u, 1] = parted[6].astype(bf)
        first_y[j, u, 0] = parted[5].astype(bf)
        first_y[j, u, 1] = parted[7].astype(bf)
        own_s[j, u, 0] = parted[0]
        own_s[j, u, 1] = parted[1]
        later_s[j, u, 0] = parted[3]
        later_s[j, u, 1] = parted[4]
        first_out(j, u, 1).start()
        first_out(j, u, 2).start()

    def pass_above(j, u):
        landed(got_x.at[j, u], f_recv.at[j, u, 0])
        second_y[j, u] = (later_s[j, u, 1] + got_x[j, u, 1].astype(jnp.float32)).astype(bf)
        second_out(j, u, 2).start()

    def pass_beside(j, u):
        landed(got_y.at[j, u], f_recv.at[j, u, 1])
        second_x[j, u] = (later_s[j, u, 0] + got_y[j, u, 1].astype(jnp.float32)).astype(bf)
        second_out(j, u, 1).start()

    def finish(j, u):
        landed(more_y.at[j, u], s_recv.at[j, u, 1])
        landed(more_x.at[j, u], s_recv.at[j, u, 0])
        final[j, pl.ds(u * half, quarter)] = (
            own_s[j, u, 0] + got_x[j, u, 0].astype(jnp.float32) + more_y[j, u].astype(jnp.float32)
        ).astype(bf)
        final[j, pl.ds(u * half + quarter, quarter)] = (
            own_s[j, u, 1] + got_y[j, u, 0].astype(jnp.float32) + more_x[j, u].astype(jnp.float32)
        ).astype(bf)

        @pl.when(jnp.logical_not(mine(j)))
        def _():
            home_out(j, u).start()

        @pl.when(mine(j))
        def _():
            pltpu.make_async_copy(
                final_rows(j, u), out_rows(me_fs, u), home_recv.at[me_fs, u]
            ).start()

    def slot(i):
        if i == 0:
            return me_sp
        return i - 1 + (i - 1 >= me_sp).astype(jnp.int32)

    state_s[...] = jnp.zeros_like(state_s)
    order = [slot(i) for i in range(planes)]
    forward_rows(3)
    forward_rows(1)
    arrive(order[0])
    forward_small()
    relay(order[0], 1)
    relay(order[0], 2)
    forward_rows(2)
    pass_across(order[0], 1)
    arrive(order[1])
    pass_across(order[0], 2)
    pass_half(order[0], 2)
    arrive(order[3])
    pass_half(order[0], 1)
    complete(order[0])
    relay(order[1], 1)
    for load in loads[2:]:
        load.wait()
    project_rows(order[0])
    relay(order[1], 2)
    arrive(order[2])
    pass_across(order[1], 1)
    relay(order[3], 1)
    relay(order[3], 2)
    project_soft(order[0])
    pass_half(order[1], 1)
    pass_across(order[3], 2)
    pass_half(order[1], 2)
    pass_across(order[1], 2)
    relay(order[2], 2)
    relay(order[2], 1)
    complete(order[1])
    project_rows(order[1])
    project_soft(order[1])
    attend_rows(0)
    pass_half(order[3], 1)
    pass_across(order[3], 1)
    pass_across(order[2], 1)
    pass_half(order[3], 2)
    pass_across(order[2], 2)
    pass_half(order[2], 2)
    pass_half(order[2], 1)
    advance_rows(0)
    mix_out(0).start()
    complete(order[3])
    complete(order[2])
    project_rows(order[2])
    project_soft(order[2])
    advance_rows(1)
    for load in out_loads:
        load.wait()
    for give in out_gives:
        give.wait_recv()
    leave(0, 0)
    leave(0, 1)
    attend_rows(1)
    mix_out(1).start()
    project_rows(order[3])
    project_soft(order[3])
    leave(1, 0)
    advance_rows(2)
    leave(1, 1)
    pass_above(0, 0)
    pass_beside(0, 0)
    attend_rows(3)
    pass_beside(0, 1)
    advance_rows(3)
    mix_out(3).start()
    attend_rows(2)
    mix_out(2).start()
    pass_above(1, 1)
    pass_beside(1, 1)
    leave(3, 0)
    leave(2, 0)
    leave(3, 1)
    pass_beside(3, 0)
    pass_above(3, 0)
    pass_above(0, 1)
    pass_beside(2, 0)
    pass_above(2, 0)
    pass_above(1, 0)
    leave(2, 1)
    finish(1, 1)
    pass_beside(1, 0)
    pass_above(3, 1)
    finish(3, 0)
    pass_beside(3, 1)
    finish(0, 1)
    finish(2, 0)
    pass_above(2, 1)
    finish(0, 0)
    finish(1, 0)
    pass_beside(2, 1)
    finish(3, 1)
    finish(2, 1)
    for p in range(planes):
        landed(mass_in.at[p], mrecv.at[p])
        all_mass_ref[:, p, :] = mass_in[p]
        mix_out(p).wait_send()
        for r in range(5):
            across(p, r).wait_send()
        for r in (1, 2):
            near_copy(p, r, 0).wait_send()
            near_copy(p, r, 1).wait_send()
            half_copy(p, r).wait_send()
            for u in range(2):
                first_out(p, u, r).wait_send()
                second_out(p, u, r).wait_send()

        @pl.when(p != me_sp)
        def _():
            mass_out(p).wait_send()

        @pl.when(jnp.logical_not(mine(p)))
        def _():
            home_out(p, 0).wait_send()
            home_out(p, 1).wait_send()

    for give in out_gives:
        give.wait_send()

    @pl.when(jnp.logical_not(home))
    def _():
        for h in range(2):
            rows_on(0, h).wait_send()
        shift_on(0).wait_send()

    for r in (1, 2, 3):
        for h in range(2):
            rows_out(r, h).wait_send()
        shift_out(r).wait_send()

        @pl.when(columns[r] != me_sp)
        def _():
            for h in range(2):
                rows_on(r, h).wait_send()
            shift_on(r).wait_send()

    for c in range(count):
        for u in range(2):
            landed(out_rows(c, u), home_recv.at[c, u])


def turned_shards(
    sizes,
    tokens,
    norm_gain,
    lin_query,
    lin_key,
    lin_value,
    lin_decay,
    decay_bias,
    decay_shift,
    soft_query,
    soft_key,
    soft_value,
    soft_lambda,
    lin_gain,
    soft_gain,
    lin_out,
    soft_out,
):
    rows, width = tokens.shape[1:]
    planes, count, parts = sizes["sp"], sizes["fs"], sizes["tp"]
    piece = rows // count
    half, quarter = piece // 2, piece // 4
    length = planes * rows
    bf, f32 = jnp.bfloat16, jnp.float32
    vmem = pl.BlockSpec(memory_space=pltpu.VMEM)
    dma = pltpu.SemaphoreType.DMA
    cos, sin = turn_tables(length)
    weights = (
        tokens[0], decay_shift[:, 0, :], norm_gain[None], decay_bias[None], soft_lambda[None],
        lin_gain[None], soft_gain[None],
        lin_query, lin_key, lin_decay, lin_value, jnp.asarray(cos), jnp.asarray(sin),
        soft_query, soft_key, soft_value, jnp.asarray(level_sums(CHUNK), bf),
    )
    mixed, all_mass = pl.pallas_call(
        functools.partial(layer_kernel, sizes),
        out_shape=(
            jax.ShapeDtypeStruct((count, piece, width), bf),
            jax.ShapeDtypeStruct((2, planes, rows), f32),
        ),
        in_specs=[pl.BlockSpec(memory_space=pl.ANY)] * (WEIGHTS + 2),
        out_specs=[vmem] * 2,
        scratch_shapes=[pltpu.VMEM(w.shape, w.dtype) for w in weights]
        + [
            pltpu.VMEM((2, GLA_VALUE + DIFF_VALUE, width), bf),
            pltpu.VMEM((planes, count, parts, piece, width), bf),
            pltpu.VMEM((planes, 2, rows), bf),
            pltpu.VMEM((rows, parts * width), bf),
            pltpu.VMEM((length, GLA_KEY), bf),
            pltpu.VMEM((length, GLA_KEY), bf),
            pltpu.VMEM((length, GLA_VALUE), bf),
            pltpu.VMEM((length, GLA_KEY), f32),
            pltpu.VMEM((length, 2 * DIFF_HEAD), bf),
            pltpu.VMEM((length, 2 * DIFF_HEAD), bf),
            pltpu.VMEM((length, DIFF_VALUE), bf),
            pltpu.VMEM((GLA_VALUE, GLA_KEY), f32),
            pltpu.VMEM((length, GLA_VALUE + DIFF_VALUE), bf),
            pltpu.VMEM((length, GLA_VALUE + DIFF_VALUE), bf),
            pltpu.VMEM((planes, 2, rows), f32),
            pltpu.VMEM((planes, 2, rows), f32),
            pltpu.VMEM((count - 1, 2, half, width), bf),
            pltpu.VMEM((count - 1, 2, rows), bf),
            pltpu.VMEM((planes, 2, 2, quarter, width), f32),
            pltpu.VMEM((planes, 2, 2, quarter, width), f32),
            pltpu.VMEM((planes, 2, 2, quarter, width), bf),
            pltpu.VMEM((planes, 2, 2, quarter, width), bf),
            pltpu.VMEM((planes, 2, 2, quarter, width), bf),
            pltpu.VMEM((planes, 2, 2, quarter, width), bf),
            pltpu.VMEM((planes, 2, quarter, width), bf),
            pltpu.VMEM((planes, 2, quarter, width), bf),
            pltpu.VMEM((planes, 2, quarter, width), bf),
            pltpu.VMEM((planes, 2, quarter, width), bf),
            pltpu.VMEM((planes, piece, width), bf),
            dma((WEIGHTS,)), dma((2,)), dma((2,)), dma((2,)),
            dma((count - 1, 2)), dma((count - 1, 2)), dma((count, 2)), dma((planes, 2)),
            dma((count - 1,)), dma((count - 1,)), dma((count,)), dma((planes,)),
            dma((planes, 2, 2)), dma((planes, 2, 2)), dma((planes, 2)), dma((planes, 2)),
            dma((planes, 5)), dma((planes, 5)), dma((planes,)), dma((planes,)),
            dma((planes, 2, 2)), dma((planes, 2, 2)), dma((planes, 2, 2)), dma((planes, 2, 2)),
            dma((planes, 2)), dma((count, 2)), dma((planes,)), dma((planes,)),
        ],
        compiler_params=pltpu.CompilerParams(
            has_side_effects=True, collective_id=0, vmem_limit_bytes=60 * 1024 * 1024
        ),
        name="whole_layer",
    )(
        *weights, lin_out, soft_out,
    )
    return mixed.reshape(1, rows, width), all_mass[None]


def solution(mesh):
    in_specs = (
        P("fs", "sp", "tp"),
        P(),
        P(None, ("fs", "tp")),
        P(None, ("fs", "tp")),
        P(None, ("fs", "tp")),
        P(None, ("fs", "tp")),
        P(),
        P(None, "fs", "sp"),
        P(None, ("fs", "tp")),
        P(None, ("fs", "tp")),
        P(None, ("fs", "tp")),
        P(),
        P(),
        P(),
        P(("fs", "tp"), None),
        P(("fs", "tp"), None),
    )
    out_specs = (P("fs", "sp", "tp"), P(("fs", "tp"), None, None, "sp"))
    sizes = dict(mesh.shape)

    def per_device(*args):
        one_head = args[2].shape[1] == GLA_KEY and args[10].shape[1] == DIFF_VALUE
        square = sizes["fs"] == sizes["sp"] == 4 and sizes["tp"] == 2 and args[0].shape[0] == 1
        if one_head and square:
            return turned_shards(sizes, *args)
        return shards(*args)

    return jax.shard_map(per_device, mesh=mesh, in_specs=in_specs, out_specs=out_specs, check_vma=False)
```

```python
import functools

import jax
import jax.numpy as jnp
import numpy as np
from jax import lax
from jax.experimental import pallas as pl
from jax.experimental.pallas import tpu as pltpu
from jax.sharding import PartitionSpec as P

GLA_KEY = 128
GLA_VALUE = 256
DIFF_HEAD = 128
DIFF_VALUE = 256
BLOCK = 64


norm_eps = 1e-06
decay_tau = 16.0
rope_base = 500000.0
highest = lax.Precision.HIGHEST


def prefix(array, axis, join, neutral):
    place = lax.axis_index(axis)
    gathered = jax.tree.map(
        lambda a, kind: lax.all_gather(a.astype(kind), axis), array, (jnp.bfloat16, jnp.bfloat16)
    )
    state = jax.tree.map(lambda a, e: jnp.zeros_like(a) + jnp.asarray(e, a.dtype), array, neutral)

    def one(turn, state):
        return join(
            state,
            jax.tree.map(
                lambda a, own: lax.dynamic_index_in_dim(a, turn, 0, False).astype(own.dtype),
                gathered,
                array,
            ),
        )

    return lax.fori_loop(0, place, one, state)


def scaled_rms(values, norm_gain):
    return (
        values * lax.rsqrt(jnp.mean(values * values, axis=-1, keepdims=True) + norm_eps) * norm_gain
    )


def rotate(values, positions):
    half_dim = values.shape[-1] // 2
    inv_freq = jnp.power(
        jnp.float32(rope_base), -jnp.arange(half_dim, dtype=jnp.float32) * (2.0 / values.shape[-1])
    )
    angles = positions.astype(jnp.float32)[:, None] * inv_freq[None, :]
    cos_table = jnp.cos(angles)[:, None, None, :]
    sin_table = jnp.sin(angles)[:, None, None, :]
    widened = values.astype(jnp.float32)
    first_half = widened[..., :half_dim]
    second_half = widened[..., half_dim:]
    turned = jnp.concatenate(
        [
            first_half * cos_table - second_half * sin_table,
            second_half * cos_table + first_half * sin_table,
        ],
        axis=-1,
    )
    return turned.astype(jnp.bfloat16)


def block_pass(queries, key_rows, value_rows, log_decay, block_len):
    groups, length, heads, key_dim = queries.shape
    value_dim = value_rows.shape[-1]
    block_count = length // block_len

    def split(tensor):
        return tensor.reshape(groups, block_count, block_len, heads, tensor.shape[-1]).transpose(
            1, 0, 3, 2, 4
        )

    causal = jnp.tril(jnp.ones((block_len, block_len), dtype=bool))[:, :, None]

    def advance(carry, inputs):
        state_now, offset = carry
        query_blk, key_blk, value_blk, decay_blk = inputs
        cum_log = jnp.cumsum(decay_blk, axis=2)
        inner_part = jnp.einsum(
            "bhcd,bhdv->bhcv", query_blk * jnp.exp(cum_log), state_now, precision=highest
        )
        decay_pair = jnp.exp(
            jnp.where(causal, cum_log[:, :, :, None, :] - cum_log[:, :, None, :, :], -jnp.inf)
        )
        scores = jnp.sum(
            query_blk[:, :, :, None, :] * key_blk[:, :, None, :, :] * decay_pair, axis=-1
        )
        local_part = jnp.einsum("bhij,bhjv->bhiv", scores, value_blk, precision=highest)
        last_log = cum_log[:, :, -1, :]
        state_now = jnp.exp(last_log)[..., None] * state_now + jnp.einsum(
            "bhcd,bhcv->bhdv",
            key_blk * jnp.exp(last_log[:, :, None, :] - cum_log),
            value_blk,
            precision=highest,
        )
        carried = query_blk * jnp.exp(offset[:, :, None, :] + cum_log)
        return ((state_now, offset + last_log), (inner_part + local_part, carried))

    start = (
        jnp.zeros((groups, heads, key_dim, value_dim), jnp.float32),
        jnp.zeros((groups, heads, key_dim), jnp.float32),
    )
    (state_end, offset_end), (outs, carried) = lax.scan(
        advance, start, (split(queries), split(key_rows), split(value_rows), split(log_decay))
    )
    return (outs, carried, state_end, offset_end)


def project(rows, weight):
    lead_shape = rows.shape[:-1]
    flat_rows = rows.reshape(-1, rows.shape[-1])
    product = jnp.dot(flat_rows, weight, preferred_element_type=jnp.float32)
    return product.reshape(lead_shape + (weight.shape[1],))


def chain_join(earlier, later):
    return (earlier[0] * later[0], later[0][..., None] * earlier[1] + later[1])


def attend(queries, query_pos, reach, all_keys, all_values, soft_lambda, soft_gain, rows_dev):
    groups, query_rows, soft_heads = queries.shape[:3]
    block_total = all_keys.shape[1] // rows_dev
    scale = DIFF_HEAD ** (-0.5)

    def first_pass(block_id, carry):
        top_now, total_now, score_store = carry
        key_blk = lax.dynamic_slice_in_dim(all_keys, block_id * rows_dev, rows_dev, 1)
        raw_scores = (
            jnp.einsum("bqhmd,bkhmd->bhmqk", queries, key_blk, preferred_element_type=jnp.float32)
            * scale
        )
        key_pos = block_id * rows_dev + jnp.arange(rows_dev, dtype=jnp.int32)
        scores = jnp.where(key_pos[None, :] <= query_pos[:, None], raw_scores, -jnp.inf)
        top_next = jnp.maximum(top_now, jnp.max(scores, axis=-1))
        total_next = total_now * jnp.exp(top_now - top_next) + jnp.sum(
            jnp.exp(scores - top_next[..., None]), axis=-1
        )
        score_store = lax.dynamic_update_index_in_dim(score_store, scores, block_id, 0)
        return (top_next, total_next, score_store)

    stat_shape = (groups, soft_heads, 2, query_rows)
    store_init = jnp.full((block_total,) + stat_shape + (rows_dev,), -jnp.inf, jnp.float32)
    top_all, total_all, score_store = lax.fori_loop(
        0,
        reach,
        first_pass,
        (
            jnp.full(stat_shape, -jnp.inf, jnp.float32),
            jnp.zeros(stat_shape, jnp.float32),
            store_init,
        ),
    )
    mass = top_all + jnp.log(total_all)

    def second_pass(block_id, accum):
        scores = lax.dynamic_index_in_dim(score_store, block_id, 0, keepdims=False)
        probs = jnp.exp(scores - top_all[..., None]) / total_all[..., None]
        weights = (probs[:, :, 0] - soft_lambda[None, :, None, None] * probs[:, :, 1]).astype(
            jnp.bfloat16
        )
        value_blk = lax.dynamic_slice_in_dim(all_values, block_id * rows_dev, rows_dev, 1)
        return accum + jnp.einsum(
            "bhqk,bkhv->bhqv", weights, value_blk, preferred_element_type=jnp.float32
        )

    accum = lax.fori_loop(
        0, reach, second_pass, jnp.zeros((groups, soft_heads, query_rows, DIFF_VALUE), jnp.float32)
    )
    soft_mix = scaled_rms(accum, soft_gain).astype(jnp.bfloat16).transpose(0, 2, 1, 3)
    soft_mix = soft_mix.reshape(groups, query_rows, soft_heads * DIFF_VALUE)
    return (soft_mix, mass)


def mixers(
    normed,
    shift_rows,
    lin_query,
    lin_key,
    lin_value,
    lin_decay,
    decay_bias,
    soft_query,
    soft_key,
    soft_value,
    soft_lambda,
    lin_gain,
    soft_gain,
):
    groups, rows_dev, model_width = normed.shape
    lin_heads = lin_query.shape[1] // GLA_KEY
    soft_heads = soft_value.shape[1] // DIFF_VALUE
    place = lax.axis_index("sp")
    shift_wide = shift_rows.astype(jnp.float32)
    lin_q = (
        project(normed, lin_query)
        .astype(jnp.bfloat16)
        .reshape(groups, rows_dev, lin_heads, GLA_KEY)
    )
    lin_k = (
        project(normed, lin_key).astype(jnp.bfloat16).reshape(groups, rows_dev, lin_heads, GLA_KEY)
    )
    lin_v = (
        project(normed, lin_value)
        .astype(jnp.bfloat16)
        .reshape(groups, rows_dev, lin_heads, GLA_VALUE)
    )
    gate_input = project(normed, lin_decay) + decay_bias + shift_wide[0][:, :, None]
    log_decay = jax.nn.log_sigmoid(gate_input) / decay_tau + shift_wide[1][:, :, None]
    log_decay = log_decay.reshape(groups, rows_dev, lin_heads, GLA_KEY)
    outs, carried, state_end, offset_end = block_pass(
        lin_q.astype(jnp.float32),
        lin_k.astype(jnp.float32),
        lin_v.astype(jnp.float32),
        log_decay,
        BLOCK,
    )
    keep_in, state_in = prefix(
        (jnp.exp(offset_end), state_end),
        "sp",
        chain_join,
        (jnp.ones_like(offset_end), jnp.zeros_like(state_end)),
    )
    outs = outs + jnp.einsum("nbhcd,bhdv->nbhcv", carried, state_in, precision=highest)
    lin_raw = outs.transpose(1, 0, 3, 2, 4).reshape(groups, rows_dev, lin_heads, GLA_VALUE)
    lin_mix = (
        scaled_rms(lin_raw, lin_gain)
        .astype(jnp.bfloat16)
        .reshape(groups, rows_dev, lin_heads * GLA_VALUE)
    )
    positions = place * rows_dev + jnp.arange(rows_dev, dtype=jnp.int32)
    soft_q = rotate(
        project(normed, soft_query)
        .astype(jnp.bfloat16)
        .reshape(groups, rows_dev, soft_heads, 2, DIFF_HEAD),
        positions,
    )
    soft_k = rotate(
        project(normed, soft_key)
        .astype(jnp.bfloat16)
        .reshape(groups, rows_dev, soft_heads, 2, DIFF_HEAD),
        positions,
    )
    soft_v = (
        project(normed, soft_value)
        .astype(jnp.bfloat16)
        .reshape(groups, rows_dev, soft_heads, DIFF_VALUE)
    )
    all_keys, all_values = (
        lax.all_gather(soft_k, "sp", axis=1, tiled=True),
        lax.all_gather(soft_v, "sp", axis=1, tiled=True),
    )
    soft_mix, mass = attend(
        soft_q, positions, place + 1, all_keys, all_values, soft_lambda, soft_gain, rows_dev
    )
    return (lin_mix, soft_mix, mass)


def output_term(lin_mix, soft_mix, lin_out, soft_out, rows_dev, parts):
    col_width = lin_out.shape[1] // parts

    def term(start, row_count):
        pieces = []
        for turn_index in range(row_count // rows_dev):
            piece_id = (start + turn_index * rows_dev) // rows_dev
            seq_id = piece_id // parts
            part_id = piece_id % parts
            lin_rows = lax.dynamic_index_in_dim(lin_mix, seq_id, 0, keepdims=False)
            soft_rows = lax.dynamic_index_in_dim(soft_mix, seq_id, 0, keepdims=False)
            lin_cols = lax.dynamic_slice_in_dim(lin_out, part_id * col_width, col_width, 1)
            soft_cols = lax.dynamic_slice_in_dim(soft_out, part_id * col_width, col_width, 1)
            pieces.append(
                jnp.dot(lin_rows, lin_cols, preferred_element_type=jnp.float32)
                + jnp.dot(soft_rows, soft_cols, preferred_element_type=jnp.float32)
            )
        return jnp.concatenate(pieces, axis=0)

    return term


def shards(
    tokens,
    norm_gain,
    lin_query,
    lin_key,
    lin_value,
    lin_decay,
    decay_bias,
    decay_shift,
    soft_query,
    soft_key,
    soft_value,
    soft_lambda,
    lin_gain,
    soft_gain,
    lin_out,
    soft_out,
):
    rows_dev = tokens.shape[1]
    parts = lax.axis_size("tp")
    fs_size = lax.axis_size("fs")
    fs_index = lax.axis_index("fs")
    tp_index = lax.axis_index("tp")
    whole = lax.all_gather(tokens, "tp", axis=2, tiled=True).astype(jnp.float32)
    normed = scaled_rms(whole, norm_gain).astype(jnp.bfloat16)
    lambda_grid = soft_lambda.reshape(fs_size, parts, -1)
    bias_grid = decay_bias.reshape(fs_size, parts, -1)
    all_rows, all_shift = (
        lax.all_gather(normed, "fs", axis=0, tiled=True),
        lax.all_gather(decay_shift, "fs", axis=1, tiled=True),
    )
    head_lambda = lax.dynamic_index_in_dim(
        lax.dynamic_index_in_dim(lambda_grid, fs_index, 0, keepdims=False),
        tp_index,
        0,
        keepdims=False,
    )
    head_bias = lax.dynamic_index_in_dim(
        lax.dynamic_index_in_dim(bias_grid, fs_index, 0, keepdims=False),
        tp_index,
        0,
        keepdims=False,
    )
    lin_mix, soft_mix, mass = mixers(
        all_rows,
        all_shift,
        lin_query,
        lin_key,
        lin_value,
        lin_decay,
        head_bias,
        soft_query,
        soft_key,
        soft_value,
        head_lambda,
        lin_gain,
        soft_gain,
    )
    term = output_term(lin_mix, soft_mix, lin_out, soft_out, rows_dev, parts)
    summed = lax.psum_scatter(
        term(jnp.int32(0), rows_dev * lax.axis_size(("fs", "tp"))).astype(jnp.bfloat16),
        ("fs", "tp"),
        scatter_dimension=0,
        tiled=True,
    ).astype(jnp.float32)
    log_mass = mass.transpose(1, 2, 0, 3)
    mixed = summed.astype(jnp.bfloat16).reshape(1, rows_dev, summed.shape[1])
    return (mixed, log_mass)


CHUNK = 128


def level_sums(length):
    levels = length.bit_length() - 1
    row = np.arange(length)
    spans = []
    for level in range(levels):
        half = 1 << level
        middle = (row // (2 * half)) * (2 * half) + half - 1
        low, high = np.minimum(row, middle), np.maximum(row, middle)
        spans.append((row[None, :] > low[:, None]) & (row[None, :] <= high[:, None]))
    spans.append(row[None, :] <= row[:, None])
    spans.append(row[None, :] > row[:, None])
    table = np.concatenate(spans, axis=0)
    return np.concatenate([table, table], axis=1).astype(np.float32)


def turn_tables(length):
    half = DIFF_HEAD // 2
    inv_freq = rope_base ** (-np.arange(half, dtype=np.float64) * (2.0 / DIFF_HEAD))
    angles = np.arange(length, dtype=np.float64)[:, None] * inv_freq[None, :]
    cos, sin = np.cos(angles), np.sin(angles)
    return (
        np.concatenate([cos, cos], axis=1).astype(np.float32),
        np.concatenate([-sin, sin], axis=1).astype(np.float32),
    )


def nt(a, b):
    return lax.dot_general(a, b, (((1,), (1,)), ((), ())), preferred_element_type=jnp.float32)


def tn(a, b):
    return lax.dot_general(a, b, (((0,), (0,)), ((), ())), preferred_element_type=jnp.float32)


def nn(a, b):
    return jnp.dot(a, b, preferred_element_type=jnp.float32)


WEIGHTS = 17


def layer_kernel(
    sizes,
    *refs,
):
    far = refs[:WEIGHTS]
    lo_far, so_far = refs[WEIGHTS : WEIGHTS + 2]
    out_ref, all_mass_ref = refs[WEIGHTS + 2 : WEIGHTS + 4]
    near = refs[WEIGHTS + 4 : 2 * WEIGHTS + 4]
    (
        wout_ref, x_ref, rows_ref, normed_s, q_s, k_s, v_s, dec_s, a_s, b_s, c_s, state_s, mix_s, omix_s,
        mass_ref, mass_in, via, via_shift, own_s, later_s, first_x, first_y, got_x, got_y,
        second_x, second_y, more_x, more_y, final,
        wsem, osem, wo_send, wo_recv, sc_send, via_recv, z_send, in_recv,
        sh_send, sh_recv, shz_send, shz_recv,
        g_send, g_recv, h_send, h_recv, ac_send, ac_recv, mix_send, mix_recv,
        ready, f_send, f_recv, s_send, s_recv, home_send, home_recv, msend, mrecv,
    ) = refs[2 * WEIGHTS + 4 :]
    (
        tok_ref, shift_ref, gain_ref, bias_ref, lam_ref, lgain_ref, sgain_ref,
        lq_ref, lk_ref, ld_ref, lv_ref, cos_ref, sin_ref, sq_ref, sk_ref, sv_ref, span_ref,
    ) = near
    planes, count, parts, piece, width = x_ref.shape
    rows = count * piece
    half, quarter = piece // 2, piece // 4
    scale = DIFF_HEAD ** (-0.5)
    bf = jnp.bfloat16
    me_sp, me_fs, me_tp = lax.axis_index("sp"), lax.axis_index("fs"), lax.axis_index("tp")
    other = 1 - me_tp
    home = me_sp == me_fs
    low, high_bit = me_fs % 2, me_fs // 2
    beside = high_bit * 2 + 1 - low
    above = (1 - high_bit) * 2 + low
    across_from = (1 - high_bit) * 2 + 1 - low
    columns = (me_fs, beside, above, across_from)

    def remote(src, dst, send, recv, sp, fs, tp):
        return pltpu.make_async_remote_copy(
            src_ref=src,
            dst_ref=dst,
            send_sem=send,
            recv_sem=recv,
            device_id={"sp": sp, "fs": fs, "tp": tp},
            device_id_type=pl.DeviceIdType.MESH,
        )

    def landed(ref, sem):
        pltpu.make_async_copy(ref, ref, sem).wait()

    def piece_of(c, h=0, count_of=2):
        return tok_ref.at[pl.ds(pl.multiple_of(c * piece + h * half, half), count_of * half)]

    def rows_out(r, h):
        return remote(
            piece_of(columns[r], h, 1), via.at[r - 1, h],
            sc_send.at[r - 1, h], via_recv.at[r - 1, h], me_sp, columns[r], me_tp,
        )

    def rows_home(r, h):
        c = columns[r]
        return remote(
            piece_of(c, h, 1), x_ref.at[me_sp, c, me_tp, pl.ds(h * half, half)],
            sc_send.at[r - 1, h], in_recv.at[me_sp, h], me_sp, c, me_tp,
        )

    def rows_on(r, h):
        src = piece_of(me_fs, h, 1) if r == 0 else via.at[r - 1, h]
        return remote(
            src, x_ref.at[me_sp, me_fs, me_tp, pl.ds(h * half, half)],
            z_send.at[r, h], in_recv.at[me_sp, h], columns[r], me_fs, me_tp,
        )

    def shift_out(r):
        return remote(
            shift_ref, via_shift.at[r - 1],
            sh_send.at[r - 1], sh_recv.at[r - 1], me_sp, columns[r], me_tp,
        )

    def shift_on(r):
        src = shift_ref if r == 0 else via_shift.at[r - 1]
        return remote(
            src, rows_ref.at[me_sp], shz_send.at[r], shz_recv.at[me_sp], columns[r], me_fs, me_tp
        )

    def half_of(p, c, h):
        return x_ref.at[p, c, me_tp, pl.ds(h * half, half)]

    def near_copy(p, r, k):
        block = half_of(p, me_fs, (r - 1 + k) % 2)
        return remote(
            block, block, g_send.at[p, r - 1, k], g_recv.at[p, r - 1, k],
            me_sp, columns[r], me_tp,
        )

    def half_copy(p, r):
        block = x_ref.at[p, columns[3 - r], me_tp, pl.ds((r % 2) * half, half)]
        return remote(
            block, block, h_send.at[p, r - 1], h_recv.at[p, r - 1], me_sp, columns[r], me_tp
        )

    def across(p, r):
        if r < 3:
            block = x_ref.at[p, columns[r], me_tp]
        else:
            block = x_ref.at[p, columns[3], me_tp, pl.ds((r - 3) * half, half)]
        return remote(block, block, ac_send.at[p, r], ac_recv.at[p, r], me_sp, me_fs, other)

    def crossed(p, r):
        if r < 3:
            landed(x_ref.at[p, columns[r], other], ac_recv.at[p, r])
        else:
            landed(x_ref.at[p, columns[3], other, pl.ds((r - 3) * half, half)], ac_recv.at[p, r])

    def block_rows(j):
        return pl.ds(pl.multiple_of(j * rows, rows), rows)

    def mix_out(j):
        here = block_rows(j)
        return remote(
            mix_s.at[here], omix_s.at[here], mix_send.at[j], mix_recv.at[j], me_sp, me_fs, other
        )

    def first_out(j, u, r):
        src, dst = (first_x, got_x) if r == 1 else (first_y, got_y)
        return remote(
            src.at[j, u], dst.at[j, u], f_send.at[j, u, r - 1], f_recv.at[j, u, r - 1],
            me_sp, columns[r], me_tp,
        )

    def second_out(j, u, r):
        src, dst = (second_x, more_x) if r == 1 else (second_y, more_y)
        return remote(
            src.at[j, u], dst.at[j, u], s_send.at[j, u, r - 1], s_recv.at[j, u, r - 1],
            me_sp, columns[r], me_tp,
        )

    def final_rows(p, u):
        return final.at[p, pl.ds(u * half, half)]

    def out_rows(c, u):
        return out_ref.at[c, pl.ds(u * half, half)]

    def home_out(p, u):
        return remote(
            final_rows(p, u), out_rows(me_fs, u),
            home_send.at[p, u], home_recv.at[me_fs, u], p, me_sp, me_tp,
        )

    def mass_out(p):
        return remote(
            mass_ref.at[p], mass_in.at[me_sp], msend.at[p], mrecv.at[me_sp], p, me_fs, me_tp
        )

    def mine(p):
        return jnp.logical_and(home, p == me_sp)

    def own_cols(t):
        return pl.ds(pl.multiple_of(t * width, width), width)

    loads = [pltpu.make_async_copy(f, n, wsem.at[i]) for i, (f, n) in enumerate(zip(far, near))]
    depth = lo_far.shape[0]
    out_loads = [
        pltpu.make_async_copy(
            f.at[:, own_cols(me_tp)], wout_ref.at[0, pl.ds(i * depth, depth)], osem.at[i]
        )
        for i, f in enumerate((lo_far, so_far))
    ]
    out_gives = [
        remote(
            f.at[:, own_cols(other)], wout_ref.at[1, pl.ds(i * depth, depth)],
            wo_send.at[i], wo_recv.at[i], me_sp, me_fs, other,
        )
        for i, f in enumerate((lo_far, so_far))
    ]

    def tell(sem, sp, fs, tp):
        pl.semaphore_signal(
            sem, inc=1, device_id={"sp": sp, "fs": fs, "tp": tp},
            device_id_type=pl.DeviceIdType.MESH,
        )

    barrier = pltpu.get_barrier_semaphore()
    below, over = me_sp > 0, me_sp < planes - 1
    for c in columns[1:3]:
        tell(barrier, me_sp, c, me_tp)
    tell(barrier, me_sp, me_fs, other)

    @pl.when(below)
    def _():
        tell(barrier, me_sp - 1, me_fs, me_tp)

    @pl.when(over)
    def _():
        tell(barrier, me_sp + 1, me_fs, me_tp)

    for load in loads + out_loads:
        load.start()
    for load in loads[:2]:
        load.wait()
    pl.semaphore_wait(barrier, 3 + below.astype(jnp.int32) + over.astype(jnp.int32))

    tell(ready.at[0], me_sp, columns[2], me_tp)

    @pl.when(jnp.logical_and(below, over))
    def _():
        tell(ready.at[1], me_sp - 1, me_fs, me_tp)
        tell(ready.at[2], me_sp + 1, me_fs, me_tp)

    def far_ready():
        for steps in range(2, planes):
            up, down = me_sp + steps < planes, me_sp >= steps

            @pl.when(up)
            def _():
                pl.semaphore_wait(ready.at[2 * steps - 3], 1)

            @pl.when(down)
            def _():
                pl.semaphore_wait(ready.at[2 * steps - 2], 1)

            if steps + 1 < planes:

                @pl.when(jnp.logical_and(up, below))
                def _():
                    tell(ready.at[2 * steps - 1], me_sp - 1, me_fs, me_tp)

                @pl.when(jnp.logical_and(down, over))
                def _():
                    tell(ready.at[2 * steps], me_sp + 1, me_fs, me_tp)


    @pl.when(home)
    def _():
        for h in range(2):
            for r in (1, 2):
                rows_home(r, h).start()
            if h == 0:
                pl.semaphore_wait(ready.at[0], 1)
            rows_home(3, h).start()
            pltpu.make_async_copy(
                piece_of(me_fs, h, 1), half_of(me_sp, me_fs, h), in_recv.at[me_sp, h]
            ).start()
        pltpu.make_async_copy(shift_ref, rows_ref.at[me_sp], shz_recv.at[me_sp]).start()

    @pl.when(jnp.logical_not(home))
    def _():
        for h in range(2):
            for r in (1, 2):
                rows_out(r, h).start()
            if h == 0:
                pl.semaphore_wait(ready.at[0], 1)
            rows_out(3, h).start()
        far_ready()
        shift_on(0).start()

    @pl.when(home)
    def _():
        far_ready()

    for r in (1, 2, 3):
        shift_out(r).start()

    def goes_at(r, stage):
        target = columns[r]
        place = me_sp + (me_sp < target).astype(jnp.int32)
        return jnp.logical_and(target != me_sp, place == stage)

    def forward_rows(stage):
        @pl.when(goes_at(0, stage))
        def _():
            for h in range(2):
                rows_on(0, h).start()

        for h in range(2):
            for r in (1, 2, 3):

                @pl.when(goes_at(r, stage))
                def _():
                    landed(via.at[r - 1, h], via_recv.at[r - 1, h])
                    rows_on(r, h).start()

    def forward_shift(r):
        landed(via_shift.at[r - 1], sh_recv.at[r - 1])

        @pl.when(columns[r] != me_sp)
        def _():
            shift_on(r).start()

        @pl.when(columns[r] == me_sp)
        def _():
            pltpu.make_async_copy(
                via_shift.at[r - 1], rows_ref.at[me_sp], shz_recv.at[me_sp]
            ).start()

    def forward_small():
        for r in (1, 2, 3):
            forward_shift(r)
        for give in out_gives:
            give.start()

    def arrive(p):
        for h in range(2):
            landed(half_of(p, me_fs, h), in_recv.at[p, h])
        for k in range(2):
            near_copy(p, 1, k).start()
            near_copy(p, 2, k).start()
        across(p, 0).start()

    def relay(p, r):
        landed(half_of(p, columns[r], r - 1), g_recv.at[p, r - 1, 0])
        half_copy(p, 3 - r).start()

    def pass_across(p, r):
        landed(half_of(p, columns[r], r % 2), g_recv.at[p, r - 1, 1])
        across(p, r).start()

    def pass_half(p, r):
        landed(half_of(p, columns[3], r % 2), h_recv.at[p, r - 1])
        across(p, 3 + r % 2).start()

    def complete(p):
        for r in range(5):
            crossed(p, r)
        landed(rows_ref.at[p], shz_recv.at[p])

    head = me_fs * parts + me_tp

    def project_rows(p):
        bias = bias_ref[:, pl.ds(pl.multiple_of(head * GLA_KEY, GLA_KEY), GLA_KEY)]
        here = pl.ds(pl.multiple_of(p * rows, rows), rows)
        halves = [x_ref[p, :, t].reshape(rows, width).astype(jnp.float32) for t in range(parts)]
        square = sum(jnp.sum(h * h, axis=-1, keepdims=True) for h in halves)
        factor = lax.rsqrt(square / (parts * width) + norm_eps)
        normed = jnp.concatenate(
            [
                (h * factor * gain_ref[:, t * width : (t + 1) * width]).astype(bf)
                for t, h in enumerate(halves)
            ],
            axis=1,
        )
        normed_s[...] = normed
        qk = nn(normed, jnp.concatenate([lq_ref[...], lk_ref[...]], axis=1)).astype(bf)
        q_s[here, :] = qk[:, :GLA_KEY]
        k_s[here, :] = qk[:, GLA_KEY:]
        v_s[here, :] = nn(normed, lv_ref[...]).astype(bf)
        lane = lax.broadcasted_iota(jnp.int32, (rows_ref.shape[1], 2 * GLA_KEY), 1)
        sub = lax.broadcasted_iota(jnp.int32, (rows_ref.shape[1], 2 * GLA_KEY), 0)
        pick = jnp.where(sub == lane // GLA_KEY, 1.0, 0.0).astype(bf)
        shift = tn(rows_ref[p], pick)
        gate = nn(normed, ld_ref[...]) + bias + shift[:, :GLA_KEY]
        log_sig = jnp.minimum(gate, 0.0) - jnp.log1p(jnp.exp(-jnp.abs(gate)))
        dec_s[here, :] = log_sig * (1.0 / decay_tau) + shift[:, GLA_KEY:]

    def project_soft(p):
        here = pl.ds(pl.multiple_of(p * rows, rows), rows)
        normed = normed_s[...]
        cos, sin = cos_ref[here, :], sin_ref[here, :]
        for w_ref, dst in ((sq_ref, a_s), (sk_ref, b_s)):
            wide = nn(normed, w_ref[...]).astype(bf).astype(jnp.float32)
            for m in range(2):
                one = wide[:, m * DIFF_HEAD : (m + 1) * DIFF_HEAD]
                turned = one * cos + pltpu.roll(one, DIFF_HEAD // 2, 1) * sin
                dst[here, m * DIFF_HEAD : (m + 1) * DIFF_HEAD] = turned.astype(bf)
        c_s[here, :] = nn(normed, sv_ref[...]).astype(bf)

    levels = CHUNK.bit_length() - 1
    row = lax.broadcasted_iota(jnp.int32, (CHUNK, CHUNK), 0)
    col = lax.broadcasted_iota(jnp.int32, (CHUNK, CHUNK), 1)
    apart = row ^ col

    def advance(first):
        here = pl.ds(first, CHUNK)
        query, key, value = q_s[here, :].astype(jnp.float32), k_s[here, :].astype(jnp.float32), v_s[here, :]
        decay = dec_s[here, :]
        high = decay.astype(bf)
        low = (decay - high.astype(jnp.float32)).astype(bf)
        factors = jnp.exp(nn(span_ref[...], jnp.concatenate([high, low], axis=0)))
        scores = nt(q_s[here, :], k_s[here, :])
        for level in range(levels):
            factor = factors[level * CHUNK : (level + 1) * CHUNK]
            one = nt((query * factor).astype(bf), (key * factor).astype(bf))
            scores = jnp.where((apart >> level) == 1, one, scores)
        scores = jnp.where(row >= col, scores, 0.0).astype(bf)
        gone = factors[levels * CHUNK : (levels + 1) * CHUNK]
        left = factors[(levels + 1) * CHUNK :]
        state = state_s[...]
        raw = nn(scores, value) + nt((query * gone).astype(bf), state.astype(bf))
        state_s[...] = state * gone[CHUNK - 1 :, :] + tn(value, (key * left).astype(bf))
        norm = lax.rsqrt(jnp.mean(raw * raw, axis=-1, keepdims=True) + norm_eps)
        mix_s[here, :GLA_VALUE] = (raw * norm * lgain_ref[...]).astype(bf)

    heads_at = lax.broadcasted_iota(jnp.int32, lam_ref.shape, 1)
    rate = scale * float(np.log2(np.e))
    key_pos = lax.broadcasted_iota(jnp.int32, (rows, rows), 0)
    query_pos = lax.broadcasted_iota(jnp.int32, (rows, rows), 1)

    def attend_rows(j):
        here = slice(j * rows, (j + 1) * rows)
        spans = [slice(0, j * rows), here] if j else [here]
        pieces = []
        for m in range(2):
            lanes = slice(m * DIFF_HEAD, (m + 1) * DIFF_HEAD)
            scores = [nt(b_s[span, lanes], a_s[here, lanes]) for span in spans]
            scores[-1] = jnp.where(key_pos <= query_pos, scores[-1], -jnp.inf)
            top = functools.reduce(
                jnp.maximum, [jnp.max(one, axis=0, keepdims=True) for one in scores]
            )
            mass = [jnp.exp2((one - top) * rate) for one in scores]
            total = sum(jnp.sum(one, axis=0, keepdims=True) for one in mass)
            mass_ref[j, m : m + 1, :] = top * scale + jnp.log(total)
            pieces.append((mass, 1.0 / total))
        (one, one_rate), (two, two_rate) = pieces
        lam = jnp.sum(jnp.where(heads_at == head, lam_ref[...], 0.0), axis=1, keepdims=True)
        two_rate = lam * two_rate
        raw = sum(
            tn((u * one_rate - w * two_rate).astype(bf), c_s[span, :])
            for u, w, span in zip(one, two, spans)
        )
        norm = lax.rsqrt(jnp.mean(raw * raw, axis=-1, keepdims=True) + norm_eps)
        mix_s[here, GLA_VALUE:] = (raw * norm * sgain_ref[...]).astype(bf)

        @pl.when(j != me_sp)
        def _():
            mass_out(j).start()

        @pl.when(j == me_sp)
        def _():
            pltpu.make_async_copy(mass_ref.at[j], mass_in.at[j], mrecv.at[j]).start()

    def advance_rows(j):
        for n in range(rows // CHUNK):
            advance(j * rows + n * CHUNK)

    def leave(j, u):
        if u == 0:
            landed(omix_s.at[block_rows(j)], mix_recv.at[j])

        def turned(ref):
            starts = [pl.multiple_of(j * rows + c * piece + u * half, half) for c in columns]
            return jnp.concatenate([ref[pl.ds(start, half), :] for start in starts], axis=0)

        full = nn(turned(mix_s), wout_ref[0]) + nn(turned(omix_s), wout_ref[1])
        parted = [full[i * quarter : (i + 1) * quarter] for i in range(2 * count)]
        first_x[j, u, 0] = parted[2].astype(bf)
        first_x[j, u, 1] = parted[6].astype(bf)
        first_y[j, u, 0] = parted[5].astype(bf)
        first_y[j, u, 1] = parted[7].astype(bf)
        own_s[j, u, 0] = parted[0]
        own_s[j, u, 1] = parted[1]
        later_s[j, u, 0] = parted[3]
        later_s[j, u, 1] = parted[4]
        first_out(j, u, 1).start()
        first_out(j, u, 2).start()

    def pass_above(j, u):
        landed(got_x.at[j, u], f_recv.at[j, u, 0])
        second_y[j, u] = (later_s[j, u, 1] + got_x[j, u, 1].astype(jnp.float32)).astype(bf)
        second_out(j, u, 2).start()

    def pass_beside(j, u):
        landed(got_y.at[j, u], f_recv.at[j, u, 1])
        second_x[j, u] = (later_s[j, u, 0] + got_y[j, u, 1].astype(jnp.float32)).astype(bf)
        second_out(j, u, 1).start()

    def finish(j, u):
        landed(more_y.at[j, u], s_recv.at[j, u, 1])
        landed(more_x.at[j, u], s_recv.at[j, u, 0])
        final[j, pl.ds(u * half, quarter)] = (
            own_s[j, u, 0] + got_x[j, u, 0].astype(jnp.float32) + more_y[j, u].astype(jnp.float32)
        ).astype(bf)
        final[j, pl.ds(u * half + quarter, quarter)] = (
            own_s[j, u, 1] + got_y[j, u, 0].astype(jnp.float32) + more_x[j, u].astype(jnp.float32)
        ).astype(bf)

        @pl.when(jnp.logical_not(mine(j)))
        def _():
            home_out(j, u).start()

        @pl.when(mine(j))
        def _():
            pltpu.make_async_copy(
                final_rows(j, u), out_rows(me_fs, u), home_recv.at[me_fs, u]
            ).start()

    def slot(i):
        if i == 0:
            return me_sp
        return i - 1 + (i - 1 >= me_sp).astype(jnp.int32)

    state_s[...] = jnp.zeros_like(state_s)
    order = [slot(i) for i in range(planes)]
    forward_rows(1)
    forward_rows(3)
    arrive(order[0])
    forward_small()
    relay(order[0], 1)
    relay(order[0], 2)
    forward_rows(2)
    arrive(order[1])
    pass_across(order[0], 2)
    pass_half(order[0], 2)
    pass_across(order[0], 1)
    arrive(order[3])
    pass_half(order[0], 1)
    relay(order[1], 2)
    relay(order[1], 1)
    complete(order[0])
    for load in loads[2:]:
        load.wait()
    project_rows(order[0])
    arrive(order[2])
    project_soft(order[0])
    relay(order[3], 2)
    pass_across(order[1], 1)
    relay(order[3], 1)
    pass_across(order[1], 2)
    pass_half(order[1], 1)
    pass_half(order[1], 2)
    relay(order[2], 2)
    relay(order[2], 1)
    complete(order[1])
    project_rows(order[1])
    project_soft(order[1])
    pass_across(order[3], 1)
    pass_across(order[3], 2)
    pass_half(order[3], 1)
    pass_across(order[2], 2)
    pass_half(order[3], 2)
    pass_across(order[2], 1)
    attend_rows(0)
    pass_half(order[2], 2)
    pass_half(order[2], 1)
    advance_rows(0)
    mix_out(0).start()
    complete(order[2])
    project_rows(order[2])
    project_soft(order[2])
    complete(order[3])
    advance_rows(1)
    attend_rows(1)
    mix_out(1).start()
    for load in out_loads:
        load.wait()
    for give in out_gives:
        give.wait_recv()
    leave(0, 0)
    project_rows(order[3])
    project_soft(order[3])
    advance_rows(2)
    leave(1, 0)
    attend_rows(2)
    mix_out(2).start()
    leave(0, 1)
    advance_rows(3)
    leave(2, 0)
    leave(2, 1)
    attend_rows(3)
    mix_out(3).start()
    pass_above(1, 0)
    leave(1, 1)
    leave(3, 0)
    pass_beside(2, 0)
    pass_beside(1, 0)
    pass_above(2, 0)
    leave(3, 1)
    pass_above(0, 0)
    pass_beside(0, 0)
    pass_beside(3, 0)
    pass_above(3, 0)
    finish(2, 0)
    pass_above(0, 1)
    pass_beside(0, 1)
    pass_above(1, 1)
    finish(1, 0)
    pass_beside(3, 1)
    pass_beside(1, 1)
    pass_above(3, 1)
    pass_beside(2, 1)
    finish(0, 0)
    pass_above(2, 1)
    finish(3, 0)
    finish(0, 1)
    finish(3, 1)
    finish(1, 1)
    finish(2, 1)
    for p in range(planes):
        landed(mass_in.at[p], mrecv.at[p])
        all_mass_ref[:, p, :] = mass_in[p]
        mix_out(p).wait_send()
        for r in range(5):
            across(p, r).wait_send()
        for r in (1, 2):
            near_copy(p, r, 0).wait_send()
            near_copy(p, r, 1).wait_send()
            half_copy(p, r).wait_send()
            for u in range(2):
                first_out(p, u, r).wait_send()
                second_out(p, u, r).wait_send()

        @pl.when(p != me_sp)
        def _():
            mass_out(p).wait_send()

        @pl.when(jnp.logical_not(mine(p)))
        def _():
            home_out(p, 0).wait_send()
            home_out(p, 1).wait_send()

    for give in out_gives:
        give.wait_send()

    @pl.when(jnp.logical_not(home))
    def _():
        for h in range(2):
            rows_on(0, h).wait_send()
        shift_on(0).wait_send()

    for r in (1, 2, 3):
        for h in range(2):
            rows_out(r, h).wait_send()
        shift_out(r).wait_send()

        @pl.when(columns[r] != me_sp)
        def _():
            for h in range(2):
                rows_on(r, h).wait_send()
            shift_on(r).wait_send()

    for c in range(count):
        for u in range(2):
            landed(out_rows(c, u), home_recv.at[c, u])


def turned_shards(
    sizes,
    tokens,
    norm_gain,
    lin_query,
    lin_key,
    lin_value,
    lin_decay,
    decay_bias,
    decay_shift,
    soft_query,
    soft_key,
    soft_value,
    soft_lambda,
    lin_gain,
    soft_gain,
    lin_out,
    soft_out,
):
    rows, width = tokens.shape[1:]
    planes, count, parts = sizes["sp"], sizes["fs"], sizes["tp"]
    piece = rows // count
    half, quarter = piece // 2, piece // 4
    length = planes * rows
    bf, f32 = jnp.bfloat16, jnp.float32
    vmem = pl.BlockSpec(memory_space=pltpu.VMEM)
    dma = pltpu.SemaphoreType.DMA
    cos, sin = turn_tables(length)
    weights = (
        tokens[0], decay_shift[:, 0, :], norm_gain[None], decay_bias[None], soft_lambda[None],
        lin_gain[None], soft_gain[None],
        lin_query, lin_key, lin_decay, lin_value, jnp.asarray(cos), jnp.asarray(sin),
        soft_query, soft_key, soft_value, jnp.asarray(level_sums(CHUNK), bf),
    )
    mixed, all_mass = pl.pallas_call(
        functools.partial(layer_kernel, sizes),
        out_shape=(
            jax.ShapeDtypeStruct((count, piece, width), bf),
            jax.ShapeDtypeStruct((2, planes, rows), f32),
        ),
        in_specs=[pl.BlockSpec(memory_space=pl.ANY)] * (WEIGHTS + 2),
        out_specs=[pl.BlockSpec(memory_space=pl.ANY), vmem],
        scratch_shapes=[pltpu.VMEM(w.shape, w.dtype) for w in weights]
        + [
            pltpu.VMEM((2, GLA_VALUE + DIFF_VALUE, width), bf),
            pltpu.VMEM((planes, count, parts, piece, width), bf),
            pltpu.VMEM((planes, 2, rows), bf),
            pltpu.VMEM((rows, parts * width), bf),
            pltpu.VMEM((length, GLA_KEY), bf),
            pltpu.VMEM((length, GLA_KEY), bf),
            pltpu.VMEM((length, GLA_VALUE), bf),
            pltpu.VMEM((length, GLA_KEY), f32),
            pltpu.VMEM((length, 2 * DIFF_HEAD), bf),
            pltpu.VMEM((length, 2 * DIFF_HEAD), bf),
            pltpu.VMEM((length, DIFF_VALUE), bf),
            pltpu.VMEM((GLA_VALUE, GLA_KEY), f32),
            pltpu.VMEM((length, GLA_VALUE + DIFF_VALUE), bf),
            pltpu.VMEM((length, GLA_VALUE + DIFF_VALUE), bf),
            pltpu.VMEM((planes, 2, rows), f32),
            pltpu.VMEM((planes, 2, rows), f32),
            pltpu.VMEM((count - 1, 2, half, width), bf),
            pltpu.VMEM((count - 1, 2, rows), bf),
            pltpu.VMEM((planes, 2, 2, quarter, width), f32),
            pltpu.VMEM((planes, 2, 2, quarter, width), f32),
            pltpu.VMEM((planes, 2, 2, quarter, width), bf),
            pltpu.VMEM((planes, 2, 2, quarter, width), bf),
            pltpu.VMEM((planes, 2, 2, quarter, width), bf),
            pltpu.VMEM((planes, 2, 2, quarter, width), bf),
            pltpu.VMEM((planes, 2, quarter, width), bf),
            pltpu.VMEM((planes, 2, quarter, width), bf),
            pltpu.VMEM((planes, 2, quarter, width), bf),
            pltpu.VMEM((planes, 2, quarter, width), bf),
            pltpu.VMEM((planes, piece, width), bf),
            dma((WEIGHTS,)), dma((2,)), dma((2,)), dma((2,)),
            dma((count - 1, 2)), dma((count - 1, 2)), dma((count, 2)), dma((planes, 2)),
            dma((count - 1,)), dma((count - 1,)), dma((count,)), dma((planes,)),
            dma((planes, 2, 2)), dma((planes, 2, 2)), dma((planes, 2)), dma((planes, 2)),
            dma((planes, 5)), dma((planes, 5)), dma((planes,)), dma((planes,)),
            pltpu.SemaphoreType.REGULAR((2 * planes - 3,)),
            dma((planes, 2, 2)), dma((planes, 2, 2)), dma((planes, 2, 2)), dma((planes, 2, 2)),
            dma((planes, 2)), dma((count, 2)), dma((planes,)), dma((planes,)),
        ],
        compiler_params=pltpu.CompilerParams(
            has_side_effects=True, collective_id=0, vmem_limit_bytes=60 * 1024 * 1024
        ),
        name="whole_layer",
    )(
        *weights, lin_out, soft_out,
    )
    return mixed.reshape(1, rows, width), all_mass[None]


def solution(mesh):
    in_specs = (
        P("fs", "sp", "tp"),
        P(),
        P(None, ("fs", "tp")),
        P(None, ("fs", "tp")),
        P(None, ("fs", "tp")),
        P(None, ("fs", "tp")),
        P(),
        P(None, "fs", "sp"),
        P(None, ("fs", "tp")),
        P(None, ("fs", "tp")),
        P(None, ("fs", "tp")),
        P(),
        P(),
        P(),
        P(("fs", "tp"), None),
        P(("fs", "tp"), None),
    )
    out_specs = (P("fs", "sp", "tp"), P(("fs", "tp"), None, None, "sp"))
    sizes = dict(mesh.shape)

    def per_device(*args):
        one_head = args[2].shape[1] == GLA_KEY and args[10].shape[1] == DIFF_VALUE
        square = sizes["fs"] == sizes["sp"] == 4 and sizes["tp"] == 2 and args[0].shape[0] == 1
        if one_head and square:
            return turned_shards(sizes, *args)
        return shards(*args)

    return jax.shard_map(per_device, mesh=mesh, in_specs=in_specs, out_specs=out_specs, check_vma=False)
```

```python
import functools

import jax
import jax.numpy as jnp
import numpy as np
from jax import lax
from jax.experimental import pallas as pl
from jax.experimental.pallas import tpu as pltpu
from jax.sharding import PartitionSpec as P

GLA_KEY = 128
GLA_VALUE = 256
DIFF_HEAD = 128
DIFF_VALUE = 256
BLOCK = 64


norm_eps = 1e-06
decay_tau = 16.0
rope_base = 500000.0
highest = lax.Precision.HIGHEST


def prefix(array, axis, join, neutral):
    place = lax.axis_index(axis)
    gathered = jax.tree.map(
        lambda a, kind: lax.all_gather(a.astype(kind), axis), array, (jnp.bfloat16, jnp.bfloat16)
    )
    state = jax.tree.map(lambda a, e: jnp.zeros_like(a) + jnp.asarray(e, a.dtype), array, neutral)

    def one(turn, state):
        return join(
            state,
            jax.tree.map(
                lambda a, own: lax.dynamic_index_in_dim(a, turn, 0, False).astype(own.dtype),
                gathered,
                array,
            ),
        )

    return lax.fori_loop(0, place, one, state)


def scaled_rms(values, norm_gain):
    return (
        values * lax.rsqrt(jnp.mean(values * values, axis=-1, keepdims=True) + norm_eps) * norm_gain
    )


def rotate(values, positions):
    half_dim = values.shape[-1] // 2
    inv_freq = jnp.power(
        jnp.float32(rope_base), -jnp.arange(half_dim, dtype=jnp.float32) * (2.0 / values.shape[-1])
    )
    angles = positions.astype(jnp.float32)[:, None] * inv_freq[None, :]
    cos_table = jnp.cos(angles)[:, None, None, :]
    sin_table = jnp.sin(angles)[:, None, None, :]
    widened = values.astype(jnp.float32)
    first_half = widened[..., :half_dim]
    second_half = widened[..., half_dim:]
    turned = jnp.concatenate(
        [
            first_half * cos_table - second_half * sin_table,
            second_half * cos_table + first_half * sin_table,
        ],
        axis=-1,
    )
    return turned.astype(jnp.bfloat16)


def block_pass(queries, key_rows, value_rows, log_decay, block_len):
    groups, length, heads, key_dim = queries.shape
    value_dim = value_rows.shape[-1]
    block_count = length // block_len

    def split(tensor):
        return tensor.reshape(groups, block_count, block_len, heads, tensor.shape[-1]).transpose(
            1, 0, 3, 2, 4
        )

    causal = jnp.tril(jnp.ones((block_len, block_len), dtype=bool))[:, :, None]

    def advance(carry, inputs):
        state_now, offset = carry
        query_blk, key_blk, value_blk, decay_blk = inputs
        cum_log = jnp.cumsum(decay_blk, axis=2)
        inner_part = jnp.einsum(
            "bhcd,bhdv->bhcv", query_blk * jnp.exp(cum_log), state_now, precision=highest
        )
        decay_pair = jnp.exp(
            jnp.where(causal, cum_log[:, :, :, None, :] - cum_log[:, :, None, :, :], -jnp.inf)
        )
        scores = jnp.sum(
            query_blk[:, :, :, None, :] * key_blk[:, :, None, :, :] * decay_pair, axis=-1
        )
        local_part = jnp.einsum("bhij,bhjv->bhiv", scores, value_blk, precision=highest)
        last_log = cum_log[:, :, -1, :]
        state_now = jnp.exp(last_log)[..., None] * state_now + jnp.einsum(
            "bhcd,bhcv->bhdv",
            key_blk * jnp.exp(last_log[:, :, None, :] - cum_log),
            value_blk,
            precision=highest,
        )
        carried = query_blk * jnp.exp(offset[:, :, None, :] + cum_log)
        return ((state_now, offset + last_log), (inner_part + local_part, carried))

    start = (
        jnp.zeros((groups, heads, key_dim, value_dim), jnp.float32),
        jnp.zeros((groups, heads, key_dim), jnp.float32),
    )
    (state_end, offset_end), (outs, carried) = lax.scan(
        advance, start, (split(queries), split(key_rows), split(value_rows), split(log_decay))
    )
    return (outs, carried, state_end, offset_end)


def project(rows, weight):
    lead_shape = rows.shape[:-1]
    flat_rows = rows.reshape(-1, rows.shape[-1])
    product = jnp.dot(flat_rows, weight, preferred_element_type=jnp.float32)
    return product.reshape(lead_shape + (weight.shape[1],))


def chain_join(earlier, later):
    return (earlier[0] * later[0], later[0][..., None] * earlier[1] + later[1])


def attend(queries, query_pos, reach, all_keys, all_values, soft_lambda, soft_gain, rows_dev):
    groups, query_rows, soft_heads = queries.shape[:3]
    block_total = all_keys.shape[1] // rows_dev
    scale = DIFF_HEAD ** (-0.5)

    def first_pass(block_id, carry):
        top_now, total_now, score_store = carry
        key_blk = lax.dynamic_slice_in_dim(all_keys, block_id * rows_dev, rows_dev, 1)
        raw_scores = (
            jnp.einsum("bqhmd,bkhmd->bhmqk", queries, key_blk, preferred_element_type=jnp.float32)
            * scale
        )
        key_pos = block_id * rows_dev + jnp.arange(rows_dev, dtype=jnp.int32)
        scores = jnp.where(key_pos[None, :] <= query_pos[:, None], raw_scores, -jnp.inf)
        top_next = jnp.maximum(top_now, jnp.max(scores, axis=-1))
        total_next = total_now * jnp.exp(top_now - top_next) + jnp.sum(
            jnp.exp(scores - top_next[..., None]), axis=-1
        )
        score_store = lax.dynamic_update_index_in_dim(score_store, scores, block_id, 0)
        return (top_next, total_next, score_store)

    stat_shape = (groups, soft_heads, 2, query_rows)
    store_init = jnp.full((block_total,) + stat_shape + (rows_dev,), -jnp.inf, jnp.float32)
    top_all, total_all, score_store = lax.fori_loop(
        0,
        reach,
        first_pass,
        (
            jnp.full(stat_shape, -jnp.inf, jnp.float32),
            jnp.zeros(stat_shape, jnp.float32),
            store_init,
        ),
    )
    mass = top_all + jnp.log(total_all)

    def second_pass(block_id, accum):
        scores = lax.dynamic_index_in_dim(score_store, block_id, 0, keepdims=False)
        probs = jnp.exp(scores - top_all[..., None]) / total_all[..., None]
        weights = (probs[:, :, 0] - soft_lambda[None, :, None, None] * probs[:, :, 1]).astype(
            jnp.bfloat16
        )
        value_blk = lax.dynamic_slice_in_dim(all_values, block_id * rows_dev, rows_dev, 1)
        return accum + jnp.einsum(
            "bhqk,bkhv->bhqv", weights, value_blk, preferred_element_type=jnp.float32
        )

    accum = lax.fori_loop(
        0, reach, second_pass, jnp.zeros((groups, soft_heads, query_rows, DIFF_VALUE), jnp.float32)
    )
    soft_mix = scaled_rms(accum, soft_gain).astype(jnp.bfloat16).transpose(0, 2, 1, 3)
    soft_mix = soft_mix.reshape(groups, query_rows, soft_heads * DIFF_VALUE)
    return (soft_mix, mass)


def mixers(
    normed,
    shift_rows,
    lin_query,
    lin_key,
    lin_value,
    lin_decay,
    decay_bias,
    soft_query,
    soft_key,
    soft_value,
    soft_lambda,
    lin_gain,
    soft_gain,
):
    groups, rows_dev, model_width = normed.shape
    lin_heads = lin_query.shape[1] // GLA_KEY
    soft_heads = soft_value.shape[1] // DIFF_VALUE
    place = lax.axis_index("sp")
    shift_wide = shift_rows.astype(jnp.float32)
    lin_q = (
        project(normed, lin_query)
        .astype(jnp.bfloat16)
        .reshape(groups, rows_dev, lin_heads, GLA_KEY)
    )
    lin_k = (
        project(normed, lin_key).astype(jnp.bfloat16).reshape(groups, rows_dev, lin_heads, GLA_KEY)
    )
    lin_v = (
        project(normed, lin_value)
        .astype(jnp.bfloat16)
        .reshape(groups, rows_dev, lin_heads, GLA_VALUE)
    )
    gate_input = project(normed, lin_decay) + decay_bias + shift_wide[0][:, :, None]
    log_decay = jax.nn.log_sigmoid(gate_input) / decay_tau + shift_wide[1][:, :, None]
    log_decay = log_decay.reshape(groups, rows_dev, lin_heads, GLA_KEY)
    outs, carried, state_end, offset_end = block_pass(
        lin_q.astype(jnp.float32),
        lin_k.astype(jnp.float32),
        lin_v.astype(jnp.float32),
        log_decay,
        BLOCK,
    )
    keep_in, state_in = prefix(
        (jnp.exp(offset_end), state_end),
        "sp",
        chain_join,
        (jnp.ones_like(offset_end), jnp.zeros_like(state_end)),
    )
    outs = outs + jnp.einsum("nbhcd,bhdv->nbhcv", carried, state_in, precision=highest)
    lin_raw = outs.transpose(1, 0, 3, 2, 4).reshape(groups, rows_dev, lin_heads, GLA_VALUE)
    lin_mix = (
        scaled_rms(lin_raw, lin_gain)
        .astype(jnp.bfloat16)
        .reshape(groups, rows_dev, lin_heads * GLA_VALUE)
    )
    positions = place * rows_dev + jnp.arange(rows_dev, dtype=jnp.int32)
    soft_q = rotate(
        project(normed, soft_query)
        .astype(jnp.bfloat16)
        .reshape(groups, rows_dev, soft_heads, 2, DIFF_HEAD),
        positions,
    )
    soft_k = rotate(
        project(normed, soft_key)
        .astype(jnp.bfloat16)
        .reshape(groups, rows_dev, soft_heads, 2, DIFF_HEAD),
        positions,
    )
    soft_v = (
        project(normed, soft_value)
        .astype(jnp.bfloat16)
        .reshape(groups, rows_dev, soft_heads, DIFF_VALUE)
    )
    all_keys, all_values = (
        lax.all_gather(soft_k, "sp", axis=1, tiled=True),
        lax.all_gather(soft_v, "sp", axis=1, tiled=True),
    )
    soft_mix, mass = attend(
        soft_q, positions, place + 1, all_keys, all_values, soft_lambda, soft_gain, rows_dev
    )
    return (lin_mix, soft_mix, mass)


def output_term(lin_mix, soft_mix, lin_out, soft_out, rows_dev, parts):
    col_width = lin_out.shape[1] // parts

    def term(start, row_count):
        pieces = []
        for turn_index in range(row_count // rows_dev):
            piece_id = (start + turn_index * rows_dev) // rows_dev
            seq_id = piece_id // parts
            part_id = piece_id % parts
            lin_rows = lax.dynamic_index_in_dim(lin_mix, seq_id, 0, keepdims=False)
            soft_rows = lax.dynamic_index_in_dim(soft_mix, seq_id, 0, keepdims=False)
            lin_cols = lax.dynamic_slice_in_dim(lin_out, part_id * col_width, col_width, 1)
            soft_cols = lax.dynamic_slice_in_dim(soft_out, part_id * col_width, col_width, 1)
            pieces.append(
                jnp.dot(lin_rows, lin_cols, preferred_element_type=jnp.float32)
                + jnp.dot(soft_rows, soft_cols, preferred_element_type=jnp.float32)
            )
        return jnp.concatenate(pieces, axis=0)

    return term


def shards(
    tokens,
    norm_gain,
    lin_query,
    lin_key,
    lin_value,
    lin_decay,
    decay_bias,
    decay_shift,
    soft_query,
    soft_key,
    soft_value,
    soft_lambda,
    lin_gain,
    soft_gain,
    lin_out,
    soft_out,
):
    rows_dev = tokens.shape[1]
    parts = lax.axis_size("tp")
    fs_size = lax.axis_size("fs")
    fs_index = lax.axis_index("fs")
    tp_index = lax.axis_index("tp")
    whole = lax.all_gather(tokens, "tp", axis=2, tiled=True).astype(jnp.float32)
    normed = scaled_rms(whole, norm_gain).astype(jnp.bfloat16)
    lambda_grid = soft_lambda.reshape(fs_size, parts, -1)
    bias_grid = decay_bias.reshape(fs_size, parts, -1)
    all_rows, all_shift = (
        lax.all_gather(normed, "fs", axis=0, tiled=True),
        lax.all_gather(decay_shift, "fs", axis=1, tiled=True),
    )
    head_lambda = lax.dynamic_index_in_dim(
        lax.dynamic_index_in_dim(lambda_grid, fs_index, 0, keepdims=False),
        tp_index,
        0,
        keepdims=False,
    )
    head_bias = lax.dynamic_index_in_dim(
        lax.dynamic_index_in_dim(bias_grid, fs_index, 0, keepdims=False),
        tp_index,
        0,
        keepdims=False,
    )
    lin_mix, soft_mix, mass = mixers(
        all_rows,
        all_shift,
        lin_query,
        lin_key,
        lin_value,
        lin_decay,
        head_bias,
        soft_query,
        soft_key,
        soft_value,
        head_lambda,
        lin_gain,
        soft_gain,
    )
    term = output_term(lin_mix, soft_mix, lin_out, soft_out, rows_dev, parts)
    summed = lax.psum_scatter(
        term(jnp.int32(0), rows_dev * lax.axis_size(("fs", "tp"))).astype(jnp.bfloat16),
        ("fs", "tp"),
        scatter_dimension=0,
        tiled=True,
    ).astype(jnp.float32)
    log_mass = mass.transpose(1, 2, 0, 3)
    mixed = summed.astype(jnp.bfloat16).reshape(1, rows_dev, summed.shape[1])
    return (mixed, log_mass)


CHUNK = 128


def level_sums(length):
    levels = length.bit_length() - 1
    row = np.arange(length)
    spans = []
    for level in range(levels):
        half = 1 << level
        middle = (row // (2 * half)) * (2 * half) + half - 1
        low, high = np.minimum(row, middle), np.maximum(row, middle)
        spans.append((row[None, :] > low[:, None]) & (row[None, :] <= high[:, None]))
    spans.append(row[None, :] <= row[:, None])
    spans.append(row[None, :] > row[:, None])
    table = np.concatenate(spans, axis=0)
    return np.concatenate([table, table], axis=1).astype(np.float32)


def turn_tables(length):
    half = DIFF_HEAD // 2
    inv_freq = rope_base ** (-np.arange(half, dtype=np.float64) * (2.0 / DIFF_HEAD))
    angles = np.arange(length, dtype=np.float64)[:, None] * inv_freq[None, :]
    cos, sin = np.cos(angles), np.sin(angles)
    return (
        np.concatenate([cos, cos], axis=1).astype(np.float32),
        np.concatenate([-sin, sin], axis=1).astype(np.float32),
    )


def nt(a, b):
    return lax.dot_general(a, b, (((1,), (1,)), ((), ())), preferred_element_type=jnp.float32)


def tn(a, b):
    return lax.dot_general(a, b, (((0,), (0,)), ((), ())), preferred_element_type=jnp.float32)


def nn(a, b):
    return jnp.dot(a, b, preferred_element_type=jnp.float32)


WEIGHTS = 17


def layer_kernel(
    sizes,
    *refs,
):
    far = refs[:WEIGHTS]
    lo_far, so_far = refs[WEIGHTS : WEIGHTS + 2]
    out_ref, all_mass_ref = refs[WEIGHTS + 2 : WEIGHTS + 4]
    near = refs[WEIGHTS + 4 : 2 * WEIGHTS + 4]
    (
        lqkd_ref, wout_ref, x_ref, rows_ref, normed_s, factor_s, q_s, k_s, v_s, dec_s, a_s, b_s, c_s, state_s, mix_s, omix_s,
        mass_ref, mass_in, via, via_shift, own_s, later_s, first_x, first_y, got_x, got_y,
        second_x, second_y, more_x, more_y, final,
        wsem, osem, wo_send, wo_recv, sc_send, via_recv, z_send, in_recv,
        sh_send, sh_recv, shz_send, shz_recv,
        g_send, g_recv, h_send, h_recv, ac_send, ac_recv, mix_send, mix_recv,
        ready, f_send, f_recv, s_send, s_recv, home_send, home_recv, msend, mrecv,
    ) = refs[2 * WEIGHTS + 4 :]
    (
        tok_ref, shift_ref, gain_ref, bias_ref, lam_ref, lgain_ref, sgain_ref,
        _, _, _, lv_ref, cos_ref, sin_ref, sq_ref, sk_ref, sv_ref, span_ref,
    ) = near
    planes, count, parts, piece, width = x_ref.shape
    rows = count * piece
    half, quarter = piece // 2, piece // 4
    scale = DIFF_HEAD ** (-0.5)
    bf = jnp.bfloat16
    me_sp, me_fs, me_tp = lax.axis_index("sp"), lax.axis_index("fs"), lax.axis_index("tp")
    other = 1 - me_tp
    home = me_sp == me_fs
    low, high_bit = me_fs % 2, me_fs // 2
    beside = high_bit * 2 + 1 - low
    above = (1 - high_bit) * 2 + low
    across_from = (1 - high_bit) * 2 + 1 - low
    columns = (me_fs, beside, above, across_from)

    def remote(src, dst, send, recv, sp, fs, tp):
        return pltpu.make_async_remote_copy(
            src_ref=src,
            dst_ref=dst,
            send_sem=send,
            recv_sem=recv,
            device_id={"sp": sp, "fs": fs, "tp": tp},
            device_id_type=pl.DeviceIdType.MESH,
        )

    def landed(ref, sem):
        pltpu.make_async_copy(ref, ref, sem).wait()

    def piece_of(c, h=0, count_of=2):
        return tok_ref.at[pl.ds(pl.multiple_of(c * piece + h * half, half), count_of * half)]

    def rows_out(r, h):
        return remote(
            piece_of(columns[r], h, 1), via.at[r - 1, h],
            sc_send.at[r - 1, h], via_recv.at[r - 1, h], me_sp, columns[r], me_tp,
        )

    def rows_home(r, h):
        c = columns[r]
        return remote(
            piece_of(c, h, 1), x_ref.at[me_sp, c, me_tp, pl.ds(h * half, half)],
            sc_send.at[r - 1, h], in_recv.at[me_sp, h], me_sp, c, me_tp,
        )

    def rows_on(r, h):
        src = piece_of(me_fs, h, 1) if r == 0 else via.at[r - 1, h]
        return remote(
            src, x_ref.at[me_sp, me_fs, me_tp, pl.ds(h * half, half)],
            z_send.at[r, h], in_recv.at[me_sp, h], columns[r], me_fs, me_tp,
        )

    def shift_out(r):
        return remote(
            shift_ref, via_shift.at[r - 1],
            sh_send.at[r - 1], sh_recv.at[r - 1], me_sp, columns[r], me_tp,
        )

    def shift_on(r):
        src = shift_ref if r == 0 else via_shift.at[r - 1]
        return remote(
            src, rows_ref.at[me_sp], shz_send.at[r], shz_recv.at[me_sp], columns[r], me_fs, me_tp
        )

    def half_of(p, c, h):
        return x_ref.at[p, c, me_tp, pl.ds(h * half, half)]

    def near_copy(p, r, k):
        block = half_of(p, me_fs, (r - 1 + k) % 2)
        return remote(
            block, block, g_send.at[p, r - 1, k], g_recv.at[p, r - 1, k],
            me_sp, columns[r], me_tp,
        )

    def half_copy(p, r):
        block = x_ref.at[p, columns[3 - r], me_tp, pl.ds((r % 2) * half, half)]
        return remote(
            block, block, h_send.at[p, r - 1], h_recv.at[p, r - 1], me_sp, columns[r], me_tp
        )

    def across(p, r):
        if r < 3:
            block = x_ref.at[p, columns[r], me_tp]
        else:
            block = x_ref.at[p, columns[3], me_tp, pl.ds((r - 3) * half, half)]
        return remote(block, block, ac_send.at[p, r], ac_recv.at[p, r], me_sp, me_fs, other)

    def crossed(p, r):
        if r < 3:
            landed(x_ref.at[p, columns[r], other], ac_recv.at[p, r])
        else:
            landed(x_ref.at[p, columns[3], other, pl.ds((r - 3) * half, half)], ac_recv.at[p, r])

    def block_rows(j):
        return pl.ds(pl.multiple_of(j * rows, rows), rows)

    def mix_out(j):
        here = block_rows(j)
        return remote(
            mix_s.at[here], omix_s.at[here], mix_send.at[j], mix_recv.at[j], me_sp, me_fs, other
        )

    def first_out(j, u, r):
        src, dst = (first_x, got_x) if r == 1 else (first_y, got_y)
        return remote(
            src.at[j, u], dst.at[j, u], f_send.at[j, u, r - 1], f_recv.at[j, u, r - 1],
            me_sp, columns[r], me_tp,
        )

    def second_out(j, u, r):
        src, dst = (second_x, more_x) if r == 1 else (second_y, more_y)
        return remote(
            src.at[j, u], dst.at[j, u], s_send.at[j, u, r - 1], s_recv.at[j, u, r - 1],
            me_sp, columns[r], me_tp,
        )

    def final_rows(p, u):
        return final.at[p, pl.ds(u * half, half)]

    def out_rows(c, u):
        return out_ref.at[c, pl.ds(u * half, half)]

    def home_out(p, u):
        return remote(
            final_rows(p, u), out_rows(me_fs, u),
            home_send.at[p, u], home_recv.at[me_fs, u], p, me_sp, me_tp,
        )

    def mass_out(p):
        return remote(
            mass_ref.at[p], mass_in.at[me_sp], msend.at[p], mrecv.at[me_sp], p, me_fs, me_tp
        )

    def mine(p):
        return jnp.logical_and(home, p == me_sp)

    def own_cols(t):
        return pl.ds(pl.multiple_of(t * width, width), width)

    packed = [lqkd_ref.at[:, pl.ds(i * GLA_KEY, GLA_KEY)] for i in range(3)]
    targets = list(near[:7]) + packed + list(near[10:])
    loads = [pltpu.make_async_copy(f, n, wsem.at[i]) for i, (f, n) in enumerate(zip(far, targets))]
    depth = lo_far.shape[0]
    out_loads = [
        pltpu.make_async_copy(
            f.at[:, own_cols(me_tp)], wout_ref.at[0, pl.ds(i * depth, depth)], osem.at[i]
        )
        for i, f in enumerate((lo_far, so_far))
    ]
    out_gives = [
        remote(
            f.at[:, own_cols(other)], wout_ref.at[1, pl.ds(i * depth, depth)],
            wo_send.at[i], wo_recv.at[i], me_sp, me_fs, other,
        )
        for i, f in enumerate((lo_far, so_far))
    ]

    def tell(sem, sp, fs, tp):
        pl.semaphore_signal(
            sem, inc=1, device_id={"sp": sp, "fs": fs, "tp": tp},
            device_id_type=pl.DeviceIdType.MESH,
        )

    barrier = pltpu.get_barrier_semaphore()
    below, over = me_sp > 0, me_sp < planes - 1
    for c in columns[1:3]:
        tell(barrier, me_sp, c, me_tp)
    tell(barrier, me_sp, me_fs, other)

    @pl.when(below)
    def _():
        tell(barrier, me_sp - 1, me_fs, me_tp)

    @pl.when(over)
    def _():
        tell(barrier, me_sp + 1, me_fs, me_tp)

    for load in loads + out_loads:
        load.start()
    for load in loads[:2]:
        load.wait()
    pl.semaphore_wait(barrier, 3 + below.astype(jnp.int32) + over.astype(jnp.int32))

    tell(ready.at[0], me_sp, columns[2], me_tp)

    @pl.when(jnp.logical_and(below, over))
    def _():
        tell(ready.at[1], me_sp - 1, me_fs, me_tp)
        tell(ready.at[2], me_sp + 1, me_fs, me_tp)

    def far_ready():
        for steps in range(2, planes):
            up, down = me_sp + steps < planes, me_sp >= steps

            @pl.when(up)
            def _():
                pl.semaphore_wait(ready.at[2 * steps - 3], 1)

            @pl.when(down)
            def _():
                pl.semaphore_wait(ready.at[2 * steps - 2], 1)

            if steps + 1 < planes:

                @pl.when(jnp.logical_and(up, below))
                def _():
                    tell(ready.at[2 * steps - 1], me_sp - 1, me_fs, me_tp)

                @pl.when(jnp.logical_and(down, over))
                def _():
                    tell(ready.at[2 * steps], me_sp + 1, me_fs, me_tp)


    @pl.when(home)
    def _():
        for h in range(2):
            for r in (1, 2):
                rows_home(r, h).start()
            if h == 0:
                pl.semaphore_wait(ready.at[0], 1)
            rows_home(3, h).start()
            pltpu.make_async_copy(
                piece_of(me_fs, h, 1), half_of(me_sp, me_fs, h), in_recv.at[me_sp, h]
            ).start()
        pltpu.make_async_copy(shift_ref, rows_ref.at[me_sp], shz_recv.at[me_sp]).start()

    @pl.when(jnp.logical_not(home))
    def _():
        for h in range(2):
            for r in (1, 2):
                rows_out(r, h).start()
            if h == 0:
                pl.semaphore_wait(ready.at[0], 1)
            rows_out(3, h).start()
        far_ready()
        shift_on(0).start()

    @pl.when(home)
    def _():
        far_ready()

    for r in (1, 2, 3):
        shift_out(r).start()

    def goes_at(r, stage):
        target = columns[r]
        place = me_sp + (me_sp < target).astype(jnp.int32)
        return jnp.logical_and(target != me_sp, place == stage)

    def forward_rows(stage):
        @pl.when(goes_at(0, stage))
        def _():
            for h in range(2):
                rows_on(0, h).start()

        for h in range(2):
            for r in (1, 2, 3):

                @pl.when(goes_at(r, stage))
                def _():
                    landed(via.at[r - 1, h], via_recv.at[r - 1, h])
                    rows_on(r, h).start()

    def forward_shift(r):
        landed(via_shift.at[r - 1], sh_recv.at[r - 1])

        @pl.when(columns[r] != me_sp)
        def _():
            shift_on(r).start()

        @pl.when(columns[r] == me_sp)
        def _():
            pltpu.make_async_copy(
                via_shift.at[r - 1], rows_ref.at[me_sp], shz_recv.at[me_sp]
            ).start()

    def forward_small():
        for r in (1, 2, 3):
            forward_shift(r)
        for give in out_gives:
            give.start()

    def arrive(p):
        for h in range(2):
            landed(half_of(p, me_fs, h), in_recv.at[p, h])
        for k in range(2):
            near_copy(p, 1, k).start()
            near_copy(p, 2, k).start()
        across(p, 0).start()

    def relay(p, r):
        landed(half_of(p, columns[r], r - 1), g_recv.at[p, r - 1, 0])
        half_copy(p, 3 - r).start()

    def pass_across(p, r):
        landed(half_of(p, columns[r], r % 2), g_recv.at[p, r - 1, 1])
        across(p, r).start()

    def pass_half(p, r):
        landed(half_of(p, columns[3], r % 2), h_recv.at[p, r - 1])
        across(p, 3 + r % 2).start()

    def complete(p):
        for r in range(5):
            crossed(p, r)
        landed(rows_ref.at[p], shz_recv.at[p])

    head = me_fs * parts + me_tp

    def project_rows(p):
        bias = bias_ref[:, pl.ds(pl.multiple_of(head * GLA_KEY, GLA_KEY), GLA_KEY)]
        here = pl.ds(pl.multiple_of(p * rows, rows), rows)
        halves = [x_ref[p, :, t].reshape(rows, width).astype(jnp.float32) for t in range(parts)]
        scaled = jnp.concatenate(
            [
                (h * gain_ref[:, t * width : (t + 1) * width]).astype(bf)
                for t, h in enumerate(halves)
            ],
            axis=1,
        )
        normed_s[...] = scaled
        square = sum(jnp.sum(h * h, axis=-1, keepdims=True) for h in halves)
        factor = lax.rsqrt(square / (parts * width) + norm_eps)
        factor_s[...] = jnp.broadcast_to(factor, factor_s.shape)
        qkd = nn(scaled, lqkd_ref[...])
        q_s[here, :] = (qkd[:, :GLA_KEY] * factor).astype(bf)
        k_s[here, :] = (qkd[:, GLA_KEY : 2 * GLA_KEY] * factor).astype(bf)
        v_s[here, :] = (nn(scaled, lv_ref[...]) * factor).astype(bf)
        lane = lax.broadcasted_iota(jnp.int32, (rows_ref.shape[1], 2 * GLA_KEY), 1)
        sub = lax.broadcasted_iota(jnp.int32, (rows_ref.shape[1], 2 * GLA_KEY), 0)
        pick = jnp.where(sub == lane // GLA_KEY, 1.0, 0.0).astype(bf)
        shift = tn(rows_ref[p], pick)
        gate = qkd[:, 2 * GLA_KEY :] * factor + bias + shift[:, :GLA_KEY]
        log_sig = jnp.minimum(gate, 0.0) - jnp.log1p(jnp.exp(-jnp.abs(gate)))
        dec_s[here, :] = log_sig * (1.0 / decay_tau) + shift[:, GLA_KEY:]

    def project_soft(p):
        here = pl.ds(pl.multiple_of(p * rows, rows), rows)
        scaled = normed_s[...]
        factor = factor_s[...]
        cos, sin = cos_ref[here, :], sin_ref[here, :]
        for w_ref, dst in ((sq_ref, a_s), (sk_ref, b_s)):
            wide = nn(scaled, w_ref[...])
            for m in range(2):
                one = wide[:, m * DIFF_HEAD : (m + 1) * DIFF_HEAD] * factor
                one = one.astype(bf).astype(jnp.float32)
                turned = one * cos + pltpu.roll(one, DIFF_HEAD // 2, 1) * sin
                dst[here, m * DIFF_HEAD : (m + 1) * DIFF_HEAD] = turned.astype(bf)
        wide = nn(scaled, sv_ref[...])
        for m in range(2):
            lanes = slice(m * DIFF_HEAD, (m + 1) * DIFF_HEAD)
            c_s[here, lanes] = (wide[:, lanes] * factor).astype(bf)

    levels = CHUNK.bit_length() - 1
    row = lax.broadcasted_iota(jnp.int32, (CHUNK, CHUNK), 0)
    col = lax.broadcasted_iota(jnp.int32, (CHUNK, CHUNK), 1)
    apart = row ^ col

    def advance(first, factors):
        here = pl.ds(first, CHUNK)
        query, key, value = q_s[here, :].astype(jnp.float32), k_s[here, :].astype(jnp.float32), v_s[here, :]
        scores = nt(q_s[here, :], k_s[here, :])
        for level in range(levels):
            factor = factors[level * CHUNK : (level + 1) * CHUNK]
            one = nt((query * factor).astype(bf), (key * factor).astype(bf))
            scores = jnp.where((apart >> level) == 1, one, scores)
        scores = jnp.where(row >= col, scores, 0.0).astype(bf)
        gone = factors[levels * CHUNK : (levels + 1) * CHUNK]
        left = factors[(levels + 1) * CHUNK :]
        state = state_s[...]
        raw = nn(scores, value) + nt((query * gone).astype(bf), state.astype(bf))
        state_s[...] = state * gone[CHUNK - 1 :, :] + tn(value, (key * left).astype(bf))
        norm = lax.rsqrt(jnp.mean(raw * raw, axis=-1, keepdims=True) + norm_eps)
        mix_s[here, :GLA_VALUE] = (raw * norm * lgain_ref[...]).astype(bf)

    heads_at = lax.broadcasted_iota(jnp.int32, lam_ref.shape, 1)
    rate = scale * float(np.log2(np.e))
    key_pos = lax.broadcasted_iota(jnp.int32, (rows, rows), 0)
    query_pos = lax.broadcasted_iota(jnp.int32, (rows, rows), 1)

    def attend_rows(j):
        here = slice(j * rows, (j + 1) * rows)
        spans = [slice(0, j * rows), here] if j else [here]
        pieces = []
        for m in range(2):
            lanes = slice(m * DIFF_HEAD, (m + 1) * DIFF_HEAD)
            scores = [nt(b_s[span, lanes], a_s[here, lanes]) for span in spans]
            scores[-1] = jnp.where(key_pos <= query_pos, scores[-1], -jnp.inf)
            top = functools.reduce(
                jnp.maximum, [jnp.max(one, axis=0, keepdims=True) for one in scores]
            )
            mass = [jnp.exp2((one - top) * rate) for one in scores]
            total = sum(jnp.sum(one, axis=0, keepdims=True) for one in mass)
            mass_ref[j, m : m + 1, :] = top * scale + jnp.log(total)
            pieces.append((mass, 1.0 / total))
        (one, one_rate), (two, two_rate) = pieces
        lam = jnp.sum(jnp.where(heads_at == head, lam_ref[...], 0.0), axis=1, keepdims=True)
        two_rate = lam * two_rate
        raw = sum(
            tn((u * one_rate - w * two_rate).astype(bf), c_s[span, :])
            for u, w, span in zip(one, two, spans)
        )
        norm = lax.rsqrt(jnp.mean(raw * raw, axis=-1, keepdims=True) + norm_eps)
        mix_s[here, GLA_VALUE:] = (raw * norm * sgain_ref[...]).astype(bf)

        @pl.when(j != me_sp)
        def _():
            mass_out(j).start()

        @pl.when(j == me_sp)
        def _():
            pltpu.make_async_copy(mass_ref.at[j], mass_in.at[j], mrecv.at[j]).start()

    def advance_rows(j):
        chunks = rows // CHUNK
        decay = jnp.concatenate(
            [dec_s[pl.ds(j * rows + n * CHUNK, CHUNK), :] for n in range(chunks)], axis=1
        )
        high = decay.astype(bf)
        low = (decay - high.astype(jnp.float32)).astype(bf)
        factors = jnp.exp(nn(span_ref[...], jnp.concatenate([high, low], axis=0)))
        for n in range(chunks):
            advance(j * rows + n * CHUNK, factors[:, n * GLA_KEY : (n + 1) * GLA_KEY])

    def leave(j, u):
        if u == 0:
            landed(omix_s.at[block_rows(j)], mix_recv.at[j])

        def turned(ref):
            starts = [pl.multiple_of(j * rows + c * piece + u * half, half) for c in columns]
            return jnp.concatenate([ref[pl.ds(start, half), :] for start in starts], axis=0)

        full = nn(turned(mix_s), wout_ref[0]) + nn(turned(omix_s), wout_ref[1])
        parted = [full[i * quarter : (i + 1) * quarter] for i in range(2 * count)]
        first_x[j, u, 0] = parted[2].astype(bf)
        first_x[j, u, 1] = parted[6].astype(bf)
        first_y[j, u, 0] = parted[5].astype(bf)
        first_y[j, u, 1] = parted[7].astype(bf)
        own_s[j, u, 0] = parted[0]
        own_s[j, u, 1] = parted[1]
        later_s[j, u, 0] = parted[3]
        later_s[j, u, 1] = parted[4]
        first_out(j, u, 1).start()
        first_out(j, u, 2).start()

    def pass_above(j, u):
        landed(got_x.at[j, u], f_recv.at[j, u, 0])
        second_y[j, u] = (later_s[j, u, 1] + got_x[j, u, 1].astype(jnp.float32)).astype(bf)
        second_out(j, u, 2).start()

    def pass_beside(j, u):
        landed(got_y.at[j, u], f_recv.at[j, u, 1])
        second_x[j, u] = (later_s[j, u, 0] + got_y[j, u, 1].astype(jnp.float32)).astype(bf)
        second_out(j, u, 1).start()

    def finish(j, u):
        landed(more_y.at[j, u], s_recv.at[j, u, 1])
        landed(more_x.at[j, u], s_recv.at[j, u, 0])
        final[j, pl.ds(u * half, quarter)] = (
            own_s[j, u, 0] + got_x[j, u, 0].astype(jnp.float32) + more_y[j, u].astype(jnp.float32)
        ).astype(bf)
        final[j, pl.ds(u * half + quarter, quarter)] = (
            own_s[j, u, 1] + got_y[j, u, 0].astype(jnp.float32) + more_x[j, u].astype(jnp.float32)
        ).astype(bf)

        @pl.when(jnp.logical_not(mine(j)))
        def _():
            home_out(j, u).start()

        @pl.when(mine(j))
        def _():
            pltpu.make_async_copy(
                final_rows(j, u), out_rows(me_fs, u), home_recv.at[me_fs, u]
            ).start()

    def slot(i):
        if i == 0:
            return me_sp
        return i - 1 + (i - 1 >= me_sp).astype(jnp.int32)

    state_s[...] = jnp.zeros_like(state_s)
    order = [slot(i) for i in range(planes)]
    forward_rows(1)
    forward_rows(3)
    arrive(order[0])
    forward_small()
    relay(order[0], 1)
    relay(order[0], 2)
    forward_rows(2)
    arrive(order[1])
    pass_across(order[0], 2)
    pass_half(order[0], 2)
    pass_across(order[0], 1)
    arrive(order[3])
    pass_half(order[0], 1)
    relay(order[1], 2)
    relay(order[1], 1)
    complete(order[0])
    for load in loads[2:]:
        load.wait()
    project_rows(order[0])
    arrive(order[2])
    project_soft(order[0])
    relay(order[3], 2)
    pass_across(order[1], 1)
    relay(order[3], 1)
    pass_across(order[1], 2)
    pass_half(order[1], 1)
    pass_half(order[1], 2)
    relay(order[2], 2)
    relay(order[2], 1)
    complete(order[1])
    project_rows(order[1])
    project_soft(order[1])
    pass_across(order[3], 1)
    pass_across(order[3], 2)
    pass_half(order[3], 1)
    pass_across(order[2], 2)
    pass_half(order[3], 2)
    pass_across(order[2], 1)
    attend_rows(0)
    pass_half(order[2], 2)
    pass_half(order[2], 1)
    advance_rows(0)
    mix_out(0).start()
    complete(order[2])
    project_rows(order[2])
    project_soft(order[2])
    complete(order[3])
    advance_rows(1)
    attend_rows(1)
    mix_out(1).start()
    for load in out_loads:
        load.wait()
    for give in out_gives:
        give.wait_recv()
    leave(0, 0)
    project_rows(order[3])
    project_soft(order[3])
    advance_rows(2)
    leave(1, 0)
    attend_rows(2)
    mix_out(2).start()
    leave(0, 1)
    advance_rows(3)
    leave(2, 0)
    leave(2, 1)
    attend_rows(3)
    mix_out(3).start()
    pass_above(1, 0)
    leave(1, 1)
    leave(3, 0)
    pass_beside(2, 0)
    pass_beside(1, 0)
    pass_above(2, 0)
    leave(3, 1)
    pass_above(0, 0)
    pass_beside(0, 0)
    pass_beside(3, 0)
    pass_above(3, 0)
    finish(2, 0)
    pass_above(0, 1)
    pass_beside(0, 1)
    pass_above(1, 1)
    finish(1, 0)
    pass_beside(3, 1)
    pass_beside(1, 1)
    pass_above(3, 1)
    pass_beside(2, 1)
    finish(0, 0)
    pass_above(2, 1)
    finish(3, 0)
    finish(0, 1)
    finish(3, 1)
    finish(1, 1)
    finish(2, 1)
    for p in range(planes):
        landed(mass_in.at[p], mrecv.at[p])
        all_mass_ref[:, p, :] = mass_in[p]
        mix_out(p).wait_send()
        for r in range(5):
            across(p, r).wait_send()
        for r in (1, 2):
            near_copy(p, r, 0).wait_send()
            near_copy(p, r, 1).wait_send()
            half_copy(p, r).wait_send()
            for u in range(2):
                first_out(p, u, r).wait_send()
                second_out(p, u, r).wait_send()

        @pl.when(p != me_sp)
        def _():
            mass_out(p).wait_send()

        @pl.when(jnp.logical_not(mine(p)))
        def _():
            home_out(p, 0).wait_send()
            home_out(p, 1).wait_send()

    for give in out_gives:
        give.wait_send()

    @pl.when(jnp.logical_not(home))
    def _():
        for h in range(2):
            rows_on(0, h).wait_send()
        shift_on(0).wait_send()

    for r in (1, 2, 3):
        for h in range(2):
            rows_out(r, h).wait_send()
        shift_out(r).wait_send()

        @pl.when(columns[r] != me_sp)
        def _():
            for h in range(2):
                rows_on(r, h).wait_send()
            shift_on(r).wait_send()

    for c in range(count):
        for u in range(2):
            landed(out_rows(c, u), home_recv.at[c, u])


def turned_shards(
    sizes,
    tokens,
    norm_gain,
    lin_query,
    lin_key,
    lin_value,
    lin_decay,
    decay_bias,
    decay_shift,
    soft_query,
    soft_key,
    soft_value,
    soft_lambda,
    lin_gain,
    soft_gain,
    lin_out,
    soft_out,
):
    rows, width = tokens.shape[1:]
    planes, count, parts = sizes["sp"], sizes["fs"], sizes["tp"]
    piece = rows // count
    half, quarter = piece // 2, piece // 4
    length = planes * rows
    bf, f32 = jnp.bfloat16, jnp.float32
    vmem = pl.BlockSpec(memory_space=pltpu.VMEM)
    dma = pltpu.SemaphoreType.DMA
    cos, sin = turn_tables(length)
    weights = (
        tokens[0], decay_shift[:, 0, :], norm_gain[None], decay_bias[None], soft_lambda[None],
        lin_gain[None], soft_gain[None],
        lin_query, lin_key, lin_decay, lin_value, jnp.asarray(cos), jnp.asarray(sin),
        soft_query, soft_key, soft_value, jnp.asarray(level_sums(CHUNK), bf),
    )
    mixed, all_mass = pl.pallas_call(
        functools.partial(layer_kernel, sizes),
        out_shape=(
            jax.ShapeDtypeStruct((count, piece, width), bf),
            jax.ShapeDtypeStruct((2, planes, rows), f32),
        ),
        in_specs=[pl.BlockSpec(memory_space=pl.ANY)] * (WEIGHTS + 2),
        out_specs=[pl.BlockSpec(memory_space=pl.ANY), vmem],
        scratch_shapes=[
            pltpu.VMEM((16, 128) if 7 <= i < 10 else w.shape, w.dtype)
            for i, w in enumerate(weights)
        ]
        + [
            pltpu.VMEM((lin_query.shape[0], 3 * GLA_KEY), bf),
            pltpu.VMEM((2, GLA_VALUE + DIFF_VALUE, width), bf),
            pltpu.VMEM((planes, count, parts, piece, width), bf),
            pltpu.VMEM((planes, 2, rows), bf),
            pltpu.VMEM((rows, parts * width), bf),
            pltpu.VMEM((rows, DIFF_HEAD), f32),
            pltpu.VMEM((length, GLA_KEY), bf),
            pltpu.VMEM((length, GLA_KEY), bf),
            pltpu.VMEM((length, GLA_VALUE), bf),
            pltpu.VMEM((length, GLA_KEY), f32),
            pltpu.VMEM((length, 2 * DIFF_HEAD), bf),
            pltpu.VMEM((length, 2 * DIFF_HEAD), bf),
            pltpu.VMEM((length, DIFF_VALUE), bf),
            pltpu.VMEM((GLA_VALUE, GLA_KEY), f32),
            pltpu.VMEM((length, GLA_VALUE + DIFF_VALUE), bf),
            pltpu.VMEM((length, GLA_VALUE + DIFF_VALUE), bf),
            pltpu.VMEM((planes, 2, rows), f32),
            pltpu.VMEM((planes, 2, rows), f32),
            pltpu.VMEM((count - 1, 2, half, width), bf),
            pltpu.VMEM((count - 1, 2, rows), bf),
            pltpu.VMEM((planes, 2, 2, quarter, width), f32),
            pltpu.VMEM((planes, 2, 2, quarter, width), f32),
            pltpu.VMEM((planes, 2, 2, quarter, width), bf),
            pltpu.VMEM((planes, 2, 2, quarter, width), bf),
            pltpu.VMEM((planes, 2, 2, quarter, width), bf),
            pltpu.VMEM((planes, 2, 2, quarter, width), bf),
            pltpu.VMEM((planes, 2, quarter, width), bf),
            pltpu.VMEM((planes, 2, quarter, width), bf),
            pltpu.VMEM((planes, 2, quarter, width), bf),
            pltpu.VMEM((planes, 2, quarter, width), bf),
            pltpu.VMEM((planes, piece, width), bf),
            dma((WEIGHTS,)), dma((2,)), dma((2,)), dma((2,)),
            dma((count - 1, 2)), dma((count - 1, 2)), dma((count, 2)), dma((planes, 2)),
            dma((count - 1,)), dma((count - 1,)), dma((count,)), dma((planes,)),
            dma((planes, 2, 2)), dma((planes, 2, 2)), dma((planes, 2)), dma((planes, 2)),
            dma((planes, 5)), dma((planes, 5)), dma((planes,)), dma((planes,)),
            pltpu.SemaphoreType.REGULAR((2 * planes - 3,)),
            dma((planes, 2, 2)), dma((planes, 2, 2)), dma((planes, 2, 2)), dma((planes, 2, 2)),
            dma((planes, 2)), dma((count, 2)), dma((planes,)), dma((planes,)),
        ],
        compiler_params=pltpu.CompilerParams(
            has_side_effects=True, collective_id=0, vmem_limit_bytes=60 * 1024 * 1024
        ),
        name="whole_layer",
    )(
        *weights, lin_out, soft_out,
    )
    return mixed.reshape(1, rows, width), all_mass[None]


def solution(mesh):
    in_specs = (
        P("fs", "sp", "tp"),
        P(),
        P(None, ("fs", "tp")),
        P(None, ("fs", "tp")),
        P(None, ("fs", "tp")),
        P(None, ("fs", "tp")),
        P(),
        P(None, "fs", "sp"),
        P(None, ("fs", "tp")),
        P(None, ("fs", "tp")),
        P(None, ("fs", "tp")),
        P(),
        P(),
        P(),
        P(("fs", "tp"), None),
        P(("fs", "tp"), None),
    )
    out_specs = (P("fs", "sp", "tp"), P(("fs", "tp"), None, None, "sp"))
    sizes = dict(mesh.shape)

    def per_device(*args):
        one_head = args[2].shape[1] == GLA_KEY and args[10].shape[1] == DIFF_VALUE
        square = sizes["fs"] == sizes["sp"] == 4 and sizes["tp"] == 2 and args[0].shape[0] == 1
        if one_head and square:
            return turned_shards(sizes, *args)
        return shards(*args)

    return jax.shard_map(per_device, mesh=mesh, in_specs=in_specs, out_specs=out_specs, check_vma=False)
```
